512 devices in a mesh: sp: 64 (over z, y), tp: 8 (over x, core).
Axes of the slice: x: 4, y: 4, z: 16, core: 2. Of those that a mesh axis runs over, the one named last changes fastest.
Arguments:
- tokens: bfloat16 [65536, 2048], P('sp', 'tp'), may hold values from -6 to 6
- norm_gain: float32 [2048], replicated, may hold values from 0.1 to 1.9
- w_conv_a: bfloat16 [2048, 1024], P('sp', 'tp'), may hold values from -0.125 to 0.125
- w_conv_gate: bfloat16 [2048, 1024], P('sp', 'tp'), may hold values from -0.125 to 0.125
- conv_weight: float32 [31, 1024], P(None, 'tp'), may hold values from -16 to 16
- conv_gain: float32 [1024], P('tp'), may hold values from 0.1 to 1.9
- w_query: bfloat16 [2048, 512], P('sp', 'tp'), may hold values from -0.125 to 0.125
- w_key: bfloat16 [2048, 512], P('sp', 'tp'), may hold values from -0.125 to 0.125
- w_value: bfloat16 [2048, 1024], P('sp', 'tp'), may hold values from -0.125 to 0.125
- w_outgate: bfloat16 [2048, 1024], P('sp', 'tp'), may hold values from -0.125 to 0.125
- w_decay: bfloat16 [2048, 512], P('sp', 'tp'), may hold values from -0.125 to 0.125
- decay_bias: float32 [512], P('tp'), may hold values from 0 to 12
- decay_extra: float32 [65536, 512], P('sp', 'tp'), may hold values from -2 to 0
- head_gain: float32 [128], replicated, may hold values from 0.1 to 1.9
- init_state: float32 [8, 64, 128], P('tp'), may hold values from -1536 to 1536
- w_out_conv: bfloat16 [1024, 2048], P('tp', 'sp'), may hold values from -0.125 to 0.125
- w_out_gla: bfloat16 [1024, 2048], P('tp', 'sp'), may hold values from -0.125 to 0.125
Outputs:
- mixed: bfloat16 [65536, 2048], P(('sp', 'tp'))
The draws below stay inside these ranges and needn't reach their ends.
All inputs are finite; a program needn't handle non-finite values.
Results may differ from the reference program's by a relative error of at most 0.022.
Values may be sent and summed in bfloat16 or wider, within the bound.
A program may use at most 128 MiB of HBM per device.

```python
import jax
import jax.numpy as jnp
from jax import lax

D = 2048
D_CONV = 1024
HEADS = 8
HK = 64
HV = 128
KERNEL = 31
BLOCK = 64
TOK_DEV = 1024
SEQUENCE_TOKENS = 65536
GLA_K = 512
GLA_V = 1024
N_TP = 8


def draw_conv_weight(key, part):
    key_base = jax.random.fold_in(key, 0)
    base = jax.random.normal(key_base, (KERNEL, D_CONV), jnp.float32) * KERNEL ** (-0.5)
    rising = 3.0 ** (jnp.arange(D_CONV, dtype=jnp.float32) / (D_CONV - 1))
    return base * rising[None, :]


def draw_decay_bias(key, part):
    key_pick, key_fast, key_slow = jax.random.split(key, 3)
    fast_share = 0.5
    fast_head = jax.random.bernoulli(key_pick, fast_share, (HEADS,))
    fast_values = jax.random.uniform(key_fast, (HEADS, HK), jnp.float32, 0.0, 1.0)
    slow_values = jax.random.uniform(key_slow, (HEADS, HK), jnp.float32, 8.0, 12.0)
    return jnp.where(fast_head[:, None], fast_values, slow_values).reshape(HEADS * HK)


def draw_decay_extra(key, part):
    key_factor, key_location, key_width, key_channel = jax.random.split(key, 4)
    factor = jax.random.uniform(key_factor, (SEQUENCE_TOKENS // TOK_DEV, 1), jnp.float32, 1.0, 3.0)
    row_each = jnp.repeat(factor, TOK_DEV, axis=0)
    channel_index = jax.random.uniform(key_channel, (1, HEADS * HK), jnp.float32, 0.5, 1.5)
    spike_locations = jax.random.randint(key_location, (3,), 0, SEQUENCE_TOKENS)
    spike_depth = jax.random.uniform(key_width, (3, 1), jnp.float32, 0.22, 0.5)
    spike_events = (jnp.arange(SEQUENCE_TOKENS)[:, None] == spike_locations[None, :]).astype(jnp.float32)
    return -(0.4 / SEQUENCE_TOKENS) * row_each * channel_index - jnp.dot(spike_events, spike_depth)


def block_scale(rng, extent, cuts, least, high):
    def one(dim, shards_of):
        steps = jax.random.uniform(jax.random.fold_in(jax.random.fold_in(rng, 6), dim), (shards_of,), jnp.float32, least / len(cuts), high / len(cuts))
        return jnp.repeat(jnp.exp(steps), extent[dim] // shards_of).reshape((-1,) + (1,) * (len(extent) - dim - 1))

    factor_of = one(*cuts[0])
    for cut in cuts[1:]:
        factor_of = factor_of * one(*cut)
    return factor_of


def bell_draw(key, shape, scale, most, shards=(), kind=jnp.bfloat16):
    entries = jax.random.normal(key, shape, jnp.float32) * scale
    if len(shards) > 0:
        entries = block_scale(key, shape, shards, -0.22, 0.18) * entries
    return jnp.clip(entries, min=-most, max=most).astype(kind)


def setup_inputs(seed: int = 0) -> dict:
    streams_of = jax.random.split(jax.random.key(seed), 18)
    return {
        "tokens": bell_draw(streams_of[0], (SEQUENCE_TOKENS, D), 1.0, 6.0, ((0, 64), (1, 8))),
        "norm_gain": jnp.clip(1.0 + 0.18 * jax.random.normal(streams_of[1], (D,), jnp.float32), 0.1, 1.9),
        "w_conv_a": bell_draw(streams_of[2], (D, D_CONV), D ** -0.5, 0.125, ((0, 64), (1, 8))),
        "w_conv_gate": bell_draw(streams_of[3], (D, D_CONV), D ** -0.5, 0.125, ((0, 64), (1, 8))),
        "conv_weight": draw_conv_weight(jax.random.fold_in(streams_of[17], 71), 0),
        "conv_gain": jnp.clip(1.0 + 0.18 * jax.random.normal(streams_of[5], (D_CONV,), jnp.float32), 0.1, 1.9),
        "w_query": bell_draw(streams_of[6], (D, GLA_K), D ** -0.5, 0.125, ((0, 64), (1, 8))),
        "w_key": bell_draw(streams_of[7], (D, GLA_K), D ** -0.5, 0.125, ((0, 64), (1, 8))),
        "w_value": bell_draw(streams_of[8], (D, GLA_V), D ** -0.5, 0.125, ((0, 64), (1, 8))),
        "w_outgate": bell_draw(streams_of[9], (D, GLA_V), D ** -0.5, 0.125, ((0, 64), (1, 8))),
        "w_decay": bell_draw(streams_of[10], (D, GLA_K), D ** -0.5, 0.125, ((0, 64), (1, 8))),
        "decay_bias": draw_decay_bias(jax.random.fold_in(streams_of[17], 71), 0),
        "decay_extra": draw_decay_extra(jax.random.fold_in(streams_of[17], 71), 0),
        "head_gain": jnp.clip(1.0 + 0.18 * jax.random.normal(streams_of[13], (HV,), jnp.float32), 0.1, 1.9),
        "init_state": bell_draw(streams_of[14], (HEADS, HK, HV), (SEQUENCE_TOKENS ** 0.5), 1536.0, ((0, 8),), jnp.float32),
        "w_out_conv": bell_draw(streams_of[15], (D_CONV, D), (D_CONV + GLA_V) ** -0.5, 0.125, ((0, 8), (1, 64))),
        "w_out_gla": bell_draw(streams_of[16], (GLA_V, D), (D_CONV + GLA_V) ** -0.5, 0.125, ((0, 8), (1, 64))),
    }


epsilon = 1e-06
gate_divisor = 16.0
highest_precision = lax.Precision.HIGHEST

def project(hidden, weight):
    return jnp.dot(hidden, weight, preferred_element_type=jnp.float32)

def rounded(values_f32):
    return lax.optimization_barrier(values_f32.astype(jnp.bfloat16)).astype(jnp.float32)

def reference(tokens, norm_gain, w_conv_a, w_conv_gate, conv_weight, conv_gain, w_query, w_key, w_value, w_outgate, w_decay, decay_bias, decay_extra, head_gain, init_state, w_out_conv, w_out_gla):
    widened = tokens.astype(jnp.float32)
    normed = (widened * lax.rsqrt(lax.optimization_barrier(jnp.mean(widened * widened, axis=-1, keepdims=True)) + epsilon) * norm_gain).astype(jnp.bfloat16)
    conv_a = rounded(project(normed, w_conv_a))
    conv_gate = rounded(project(normed, w_conv_gate))
    query = rounded(project(normed, w_query))
    keys = rounded(project(normed, w_key))
    values = rounded(project(normed, w_value))
    out_gate = rounded(project(normed, w_outgate))
    decay_pre = project(normed, w_decay)
    gated = rounded(conv_a * jax.nn.sigmoid(conv_gate))
    padded = jnp.pad(gated, ((KERNEL - 1, 0), (0, 0)))
    conv_sum = jnp.zeros((SEQUENCE_TOKENS, D_CONV), jnp.float32)
    for tap_index in range(KERNEL):
        conv_sum = conv_sum + conv_weight[tap_index][None, :] * padded[tap_index:tap_index + SEQUENCE_TOKENS]
    mean_val = lax.optimization_barrier(jnp.mean(conv_sum, axis=-1, keepdims=True))
    square_mean = lax.optimization_barrier(jnp.mean(conv_sum * conv_sum, axis=-1, keepdims=True))
    conv_norm = (conv_sum - mean_val) * lax.rsqrt(square_mean - mean_val * mean_val + epsilon) * conv_gain
    conv_out = jax.nn.silu(conv_norm).astype(jnp.bfloat16)
    log_decay = jax.nn.log_sigmoid(decay_pre + decay_bias) / gate_divisor + decay_extra
    blocks = SEQUENCE_TOKENS // BLOCK

    def to_heads(array, width):
        return array.astype(jnp.float32).reshape(blocks, BLOCK, HEADS, width).transpose(0, 2, 1, 3)
    query_heads = to_heads(query, HK) * HK ** (-0.5)
    key_heads = to_heads(keys, HK)
    value_heads = to_heads(values, HV)
    cum_log = jnp.cumsum(to_heads(log_decay, HK), axis=2)
    block_total = cum_log[:, :, -1:, :]
    query_decayed = query_heads * jnp.exp(cum_log)
    key_inverse = key_heads * jnp.exp(-cum_log)
    key_to_end = key_heads * jnp.exp(block_total - cum_log)
    causal = jnp.tril(jnp.ones((BLOCK, BLOCK), dtype=bool))
    scores = jnp.where(causal, jnp.einsum('nhik,nhjk->nhij', query_decayed, key_inverse, precision=highest_precision), 0.0)
    within = jnp.einsum('nhij,nhjv->nhiv', scores, value_heads, precision=highest_precision)

    def advance(state_current, block_items):
        query_block, key_block, value_block, decay_block = block_items
        carried_state = jnp.einsum('yau,yub->yab', query_block, state_current, precision=highest_precision)
        state_following = state_current * decay_block[:, 0, :, None] + jnp.einsum('tie,tis->tes', key_block, value_block, precision=highest_precision)
        return (state_following, carried_state)
    final_state, carried_out = lax.scan(advance, init_state.astype(jnp.float32), (query_decayed, key_to_end, value_heads, jnp.exp(block_total)))
    attn = within + carried_out
    normal_attn = attn * lax.rsqrt(lax.optimization_barrier(jnp.mean(attn * attn, axis=-1, keepdims=True)) + epsilon) * head_gain
    normal_attn = normal_attn.transpose(0, 2, 1, 3).reshape(SEQUENCE_TOKENS, HEADS * HV)
    gla_out = (normal_attn * jax.nn.silu(out_gate)).astype(jnp.bfloat16)
    conv_share = D_CONV // N_TP
    value_share = HEADS * HV // N_TP
    totals = jnp.zeros((SEQUENCE_TOKENS, D), jnp.float32)
    for group_index in range(N_TP):
        partial_value = project(conv_out[:, group_index * conv_share:(group_index + 1) * conv_share], w_out_conv[group_index * conv_share:(group_index + 1) * conv_share])
        partial_value = partial_value + project(gla_out[:, group_index * value_share:(group_index + 1) * value_share], w_out_gla[group_index * value_share:(group_index + 1) * value_share])
        totals = totals + rounded(partial_value)
    return totals.astype(jnp.bfloat16)
```

```python
import jax
import jax.numpy as jnp
from jax import lax
from jax.experimental import pallas as pl
from jax.experimental.pallas import tpu as pltpu
from jax.sharding import Mesh
from jax.sharding import PartitionSpec as P

D = 2048
D_CONV = 1024
HK = 64
HV = 128
BLOCK = 64
ROWS = 1024
NZ, NY, NX, NC = 16, 4, 4, 2
SP = ("z", "y")
TP = ("x", "c")
SP_TP = ("z", "y", "x", "c")
RA, RM, RT = 96, 176, 240
F32, BF16 = jnp.float32, jnp.bfloat16

epsilon = 1e-06
gate_divisor = 16.0


def remote(src, dst, send, recv, **ids):
    return pltpu.make_async_remote_copy(
        src_ref=src,
        dst_ref=dst,
        send_sem=send,
        recv_sem=recv,
        device_id=ids,
        device_id_type=pl.DeviceIdType.MESH,
    )


class Mover:
    def __init__(self):
        self.sent = []

    def send(self, ref, send, recv, **ids):
        copy = remote(ref, ref, send, recv, **ids)
        copy.start()
        self.sent.append(copy)

    def drain(self):
        for copy in self.sent:
            copy.wait_send()
        self.sent = []


def arrived(ref, send, recv, **ids):
    remote(ref, ref, send, recv, **ids).wait_recv()


def pack_chunk(sp, gain, wa, wg, wq, wk, wv, wo, wd, woc, wog, G):
    row = gain[pl.ds(sp, 1), :]
    r = lax.broadcasted_iota(jnp.int32, (32, 32), 0)
    c = lax.broadcasted_iota(jnp.int32, (32, 32), 1)
    col = jnp.sum(jnp.where(r == c, jnp.broadcast_to(row, (32, 32)), 0.0), axis=1, keepdims=True)

    def scaled(ref):
        return ref[...].astype(F32) * col

    d = scaled(wd)
    G[sp, 0:32] = scaled(wv).astype(BF16)
    G[sp, 32:64] = jnp.concatenate([scaled(wq), scaled(wk)], axis=1).astype(BF16)
    G[sp, 64:96] = scaled(wa).astype(BF16)
    G[sp, 96:112] = jnp.concatenate([d[0:16], d[16:32]], axis=1).astype(BF16)
    G[sp, 112:144] = scaled(wg).astype(BF16)
    G[sp, 144:176] = scaled(wo).astype(BF16)
    G[sp, 176:208] = woc[...].astype(F32).T.astype(BF16)
    G[sp, 208:240] = wog[...].astype(F32).T.astype(BF16)


def gather(z, y, x, c, tokens, G, tok, local, sems):
    (a1s, a1r, a2s, a2r, b1s, b1r, b2s, b2r, xs, xr, ds_, dr) = sems
    sp = z * NY + y
    zr, zl = lax.rem(z + 1, NZ), lax.rem(z + NZ - 1, NZ)
    yr, yl = lax.rem(y + 1, NY), lax.rem(y + NY - 1, NY)
    xr_, xl_ = lax.rem(x + 1, NX), lax.rem(x + NX - 1, NX)
    xo = lax.rem(x + 2, NX)
    co = 1 - c
    m = Mover()

    def slab(xi, ci, half):
        col = pl.multiple_of((xi * NC + ci) * 256, 256)
        return tok.at[pl.ds(half * 512, 512), pl.ds(col, 256)]

    def zc(s):
        return lax.rem(z + s + 2 * NZ, NZ)

    own = pltpu.make_async_copy(
        tokens, tok.at[:, pl.ds(pl.multiple_of((x * NC + c) * 256, 256), 256)], local
    )
    own.start()
    barrier = pltpu.get_barrier_semaphore()
    partners = [dict(x=xr_), dict(x=xl_), dict(c=co), dict(y=yr), dict(y=yl), dict(y=lax.rem(y + 2, NY)), dict(z=zr), dict(z=zl)]
    for ids in partners:
        pl.semaphore_signal(barrier, inc=1, device_id=ids, device_id_type=pl.DeviceIdType.MESH)
    pl.semaphore_wait(barrier, len(partners))

    for d in (1, 3, 2):
        m.send(G.at[sp, 0:RA], a1s.at[d - 1], a1r.at[d - 1], y=lax.rem(y + d, NY))

    def b1(s):
        if 0 <= s < 8:
            m.send(G.at[zc(-s) * NY + y, RA:RT], b1s.at[0, s], b1r.at[0, s], z=zr)
        if 0 <= s < 7:
            m.send(G.at[zc(s) * NY + y, RA:RT], b1s.at[1, s], b1r.at[1, s], z=zl)

    def b1_in(s):
        arrived(G.at[zc(-s) * NY + y, RA:RT], b1s.at[0, 0], b1r.at[0, s - 1], z=zl)
        if s <= 7:
            arrived(G.at[zc(s) * NY + y, RA:RT], b1s.at[0, 0], b1r.at[1, s - 1], z=zr)

    def both(s):
        return [(s, -s)] if s in (0, 8) else [(s, -s), (s + 8, s)]

    def b2(s):
        for k, off in both(s):
            ref = G.at[zc(off) * NY + y, RA:RT]
            m.send(ref, b2s.at[0, k], b2r.at[0, k], y=yr)
            m.send(ref, b2s.at[1, k], b2r.at[1, k], y=yl)

    def b2_forward(s):
        for k, off in both(s):
            first = zc(off) * NY
            arrived(G.at[first + yl, RA:RT], b2s.at[0, 0], b2r.at[0, k], y=yl)
            m.send(G.at[first + yl, RA:RM], b2s.at[2, k], b2r.at[2, k], y=yr)
            arrived(G.at[first + yr, RA:RT], b2s.at[0, 0], b2r.at[1, k], y=yr)
            m.send(G.at[first + yr, RM:RT], b2s.at[3, k], b2r.at[3, k], y=yl)

    def b2_end(s):
        yo = lax.rem(y + 2, NY)
        for k, off in both(s):
            first = zc(off) * NY
            arrived(G.at[first + yo, RA:RM], b2s.at[0, 0], b2r.at[2, k], y=yl)
            arrived(G.at[first + yo, RM:RT], b2s.at[0, 0], b2r.at[3, k], y=yr)

    def a2(s, p):
        if s < 8:
            m.send(G.at[pl.ds(zc(-s) * NY + 2 * p, 2), 0:RA], a2s.at[0, s, p], a2r.at[0, s, p], z=zr)
        if s < 7:
            m.send(G.at[pl.ds(zc(s) * NY + 2 * p, 2), 0:RA], a2s.at[1, s, p], a2r.at[1, s, p], z=zl)

    def a2_in(s, p):
        arrived(G.at[pl.ds(zc(-s) * NY + 2 * p, 2), 0:RA], a2s.at[0, 0, 0], a2r.at[0, s - 1, p], z=zl)
        if s <= 7:
            arrived(G.at[pl.ds(zc(s) * NY + 2 * p, 2), 0:RA], a2s.at[0, 0, 0], a2r.at[1, s - 1, p], z=zr)

    def xsend(ref, k, **ids):
        m.send(ref, xs.at[k], xr.at[k], **ids)

    def xin(ref, k, **ids):
        arrived(ref, xs.at[0], xr.at[k], **ids)

    def pair(ref, k):
        m.send(ref, ds_.at[k], dr.at[k], c=co)

    b1(0)
    own.wait()
    xsend(slab(x, c, 0), 0, x=xr_)
    xsend(slab(x, c, 1), 1, x=xl_)
    xsend(slab(x, c, 1), 2, x=xr_)
    xsend(slab(x, c, 0), 3, x=xl_)
    pair(slab(x, c, 0), 0)
    pair(slab(x, c, 1), 1)
    b2(0)
    for d in (1, 2, 3):
        arrived(G.at[z * NY + lax.rem(y + NY - d, NY), 0:RA], a1s.at[0], a1r.at[d - 1], y=lax.rem(y + NY - d, NY))
    for p in (0, 1):
        a2(0, p)
    for s in range(1, 9):
        b1_in(s)
        b1(s)
        b2(s)
        for p in (0, 1):
            a2_in(s, p)
            a2(s, p)
        b2_forward(s - 1)
        if s == 3:
            xin(slab(xl_, c, 0), 0, x=xl_)
            xsend(slab(xl_, c, 0), 4, x=xr_)
            pair(slab(xl_, c, 0), 2)
            xin(slab(xr_, c, 1), 1, x=xr_)
            xsend(slab(xr_, c, 1), 5, x=xl_)
            pair(slab(xr_, c, 1), 3)
        if s == 6:
            xin(slab(xl_, c, 1), 2, x=xl_)
            pair(slab(xl_, c, 1), 4)
            xin(slab(xr_, c, 0), 3, x=xr_)
            pair(slab(xr_, c, 0), 5)
    b2_forward(8)
    xin(slab(xo, c, 0), 4, x=xl_)
    pair(slab(xo, c, 0), 6)
    xin(slab(xo, c, 1), 5, x=xr_)
    pair(slab(xo, c, 1), 7)
    for s in range(9):
        b2_end(s)
    arrivals = [(x, 0), (x, 1), (xl_, 0), (xr_, 1), (xl_, 1), (xr_, 0), (xo, 0), (xo, 1)]
    for k, (xi, half) in enumerate(arrivals):
        arrived(slab(xi, co, half), ds_.at[0], dr.at[k], c=co)
    m.drain()


GATHER_SEMS = [
    pltpu.SemaphoreType.DMA((3,)),
    pltpu.SemaphoreType.DMA((3,)),
    pltpu.SemaphoreType.DMA((2, 8, 2)),
    pltpu.SemaphoreType.DMA((2, 8, 2)),
    pltpu.SemaphoreType.DMA((2, 8)),
    pltpu.SemaphoreType.DMA((2, 8)),
    pltpu.SemaphoreType.DMA((4, 16)),
    pltpu.SemaphoreType.DMA((4, 16)),
    pltpu.SemaphoreType.DMA((6,)),
    pltpu.SemaphoreType.DMA((6,)),
    pltpu.SemaphoreType.DMA((8,)),
    pltpu.SemaphoreType.DMA((8,)),
]


def spread_weights(G, W):
    def step(k, _):
        rows = pl.ds(pl.multiple_of(k * 256, 256), 256)
        sps = pl.ds(k * 8, 8)
        for at, first in ((0, 64), (128, 112), (256, 0), (384, 144), (512, 32)):
            W[rows, at : at + 128] = G[sps, first : first + 32, :].reshape(256, 128)
        d = G[sps, 96:112, :].astype(F32)
        low = d[:, :, 0:64]
        high = d[:, :, 64:128]
        both = jnp.concatenate([low, high], axis=1).reshape(256, 64)
        both = jnp.concatenate([both, jnp.zeros_like(both)], axis=1)
        W[rows, 640:768] = both.astype(BF16)
        return 0

    lax.fori_loop(0, 8, step, 0)


def first_kernel(tokens, gain, wa, wg, wq, wk, wv, wo, wd, woc, wog, proj, dec, wout, G, tok, W, local, *sems):
    z, y, x, c = (lax.axis_index(n) for n in ("z", "y", "x", "c"))
    pack_chunk(z * NY + y, gain, wa, wg, wq, wk, wv, wo, wd, woc, wog, G)
    gather(z, y, x, c, tokens, G, tok, local, sems)
    spread_weights(G, W)
    wout[...] = G[:, 176:240, :]

    def block(i, _):
        rows = pl.ds(pl.multiple_of(i * 256, 256), 256)
        t = tok[rows, :]
        acc = jnp.zeros((256, 128), F32)
        for k in range(16):
            piece = t[:, k * 128 : k * 128 + 128].astype(F32)
            acc = acc + piece * piece
        scale = lax.rsqrt(jnp.sum(acc, axis=1, keepdims=True) * (1.0 / D) + epsilon)
        for n in range(3):
            part = jnp.dot(t, W[:, n * 256 : n * 256 + 256], preferred_element_type=F32) * scale
            if n < 2:
                proj[rows, n * 256 : n * 256 + 256] = part.astype(BF16)
            else:
                proj[rows, 512:640] = part[:, 0:128].astype(BF16)
                dec[rows, :] = part[:, 128:256]
        return 0

    lax.fori_loop(0, 4, block, 0)


def call_first(tokens, gain, weights):
    vm = pl.BlockSpec(memory_space=pltpu.VMEM)
    return pl.pallas_call(
        first_kernel,
        out_shape=(
            jax.ShapeDtypeStruct((ROWS, 640), BF16),
            jax.ShapeDtypeStruct((ROWS, 128), F32),
            jax.ShapeDtypeStruct((64, 64, 128), BF16),
        ),
        in_specs=[pl.BlockSpec(memory_space=pl.ANY)] + [vm] * 10,
        out_specs=(vm, vm, vm),
        scratch_shapes=[
            pltpu.VMEM((64, RT, 128), BF16),
            pltpu.VMEM((ROWS, D), BF16),
            pltpu.VMEM((D, 768), BF16),
            pltpu.SemaphoreType.DMA,
        ]
        + GATHER_SEMS,
        compiler_params=pltpu.CompilerParams(
            collective_id=0, has_side_effects=True, vmem_limit_bytes=60 * 1024 * 1024
        ),
    )(tokens, gain, *weights)


def passed_along(value, axis, steps):
    count = lax.axis_size(axis)
    first, last = (max(0, -steps), min(count, count - steps))
    return lax.ppermute(value, axis, [(source, source + steps) for source in range(first, last)])


def packed_total(arrays, axis):
    ends = [0]
    for a in arrays:
        ends.append(ends[-1] + a.size)
    array = jnp.concatenate([a.ravel() for a in arrays])
    copies = jnp.broadcast_to(array, (lax.axis_size(axis), *array.shape))
    subtotal = jnp.sum(lax.all_to_all(copies, axis, split_axis=0, concat_axis=0, tiled=True), axis=0)
    return tuple((subtotal[b:e].reshape(a.shape) for a, b, e in zip(arrays, ends, ends[1:])))


def collected_together(array, axis):
    leaves = jax.tree.leaves(array)
    order = sorted(range(len(leaves)), key=lambda k: -leaves[k].size)
    width = (1, *leaves[order[0]].shape)[-1]
    lines = [
        jnp.pad(leaves[k].reshape(-1), (0, -leaves[k].size % width)).reshape(-1, width)
        for k in order
    ]
    both, at, found = (lax.all_gather(jnp.concatenate(lines), axis), 0, {})
    for k, line in zip(order, lines):
        section = both[:, at : at + len(line)].reshape(len(both), -1)
        found[k] = section[:, : leaves[k].size].reshape(-1, *leaves[k].shape)
        at += len(line)
    numbers = iter(range(len(leaves)))
    return jax.tree.map(lambda _: found[next(numbers)], array)


def carried_in(array, axes, combine, identity):
    def fresh():
        return jax.tree.map(
            lambda part, zero: jnp.zeros_like(part) + jnp.asarray(zero, part.dtype), array, identity
        )

    before = start = fresh()
    subtotal = array
    for axis in reversed(axes):
        peers, mine = (lax.axis_size(axis), lax.axis_index(axis))
        pieces = collected_together(
            jax.tree.map(lambda part, kind: part.astype(kind), subtotal, (BF16, BF16)), axis
        )
        inside, subtotal = (start, start)
        for k in range(peers):
            passed = k < mine
            subtotal = combine(
                subtotal, jax.tree.map(lambda part, own: part[k].astype(own.dtype), pieces, array)
            )
            inside = jax.tree.map(lambda new, old: jnp.where(passed, new, old), subtotal, inside)
        before = combine(inside, before)
    return before


def conv_branch(conv_a, conv_gate, conv_weight, conv_gain):
    gated = (conv_a.astype(F32) * jax.nn.sigmoid(conv_gate.astype(F32))).astype(BF16)
    rim_rows = conv_weight.shape[0] - 1
    row_count = gated.shape[0]
    earlier = passed_along(gated[row_count - rim_rows :], SP, 1)
    extended = jnp.concatenate([earlier, gated], axis=0).astype(F32)
    conv_sum = jnp.zeros(gated.shape, F32)
    for tap_index in range(conv_weight.shape[0]):
        conv_sum = (
            conv_sum + conv_weight[tap_index][None, :] * extended[tap_index : tap_index + row_count]
        )
    row_sums, row_squares = packed_total(
        (jnp.sum(conv_sum, axis=1), jnp.sum(conv_sum * conv_sum, axis=1)), TP
    )
    mean_val = (row_sums / D_CONV)[:, None]
    square_mean = (row_squares / D_CONV)[:, None]
    conv_norm = (
        (conv_sum - mean_val) * lax.rsqrt(square_mean - mean_val * mean_val + epsilon) * conv_gain
    )
    return jax.nn.silu(conv_norm).astype(BF16)


def chain_step(earlier, later):
    return (earlier[0] * later[0], earlier[1] * later[0][:, :, None] + later[1])


def gla_branch(query, keys, values, out_gate, decay_pre, decay_bias, decay_extra, head_gain, init_state):
    row_count = query.shape[0]
    local_heads = init_state.shape[0]
    blocks = row_count // BLOCK
    log_decay = jax.nn.log_sigmoid(decay_pre + decay_bias) / gate_divisor + decay_extra

    def to_heads(array, width):
        return array.astype(F32).reshape(blocks, BLOCK, local_heads, width).transpose(0, 2, 1, 3)

    query_heads = to_heads(query, HK) * HK ** (-0.5)
    key_heads = to_heads(keys, HK)
    value_heads = to_heads(values, HV)
    cum_log = jnp.cumsum(to_heads(log_decay, HK), axis=2)
    block_total = cum_log[:, :, -1:, :]
    query_decayed = query_heads * jnp.exp(cum_log)
    key_inverse = key_heads * jnp.exp(-cum_log)
    key_to_end = key_heads * jnp.exp(block_total - cum_log)
    causal = jnp.tril(jnp.ones((BLOCK, BLOCK), dtype=bool))
    scores = jnp.where(causal, jnp.einsum("nhik,nhjk->nhij", query_decayed, key_inverse), 0.0)
    within = jnp.einsum("nhij,nhjv->nhiv", scores, value_heads)

    def advance(state_current, block_items):
        query_block, key_block, value_block, decay_block = block_items
        carried_state = jnp.einsum("yau,yub->yab", query_block, state_current)
        state_following = state_current * decay_block[:, 0, :, None] + jnp.einsum(
            "tie,tis->tes", key_block, value_block
        )
        return (state_following, carried_state)

    zero_state = jnp.zeros(init_state.shape, F32)
    local_end, carried_out = lax.scan(
        advance, zero_state, (query_decayed, key_to_end, value_heads, jnp.exp(block_total))
    )
    block_sums = block_total[:, :, 0, :]
    device_log = jnp.sum(block_sums, axis=0)
    prefix_log = jnp.cumsum(block_sums, axis=0) - block_sums
    before_decay, before_state = carried_in(
        (jnp.exp(device_log), local_end),
        SP,
        chain_step,
        (jnp.ones_like(device_log), jnp.zeros_like(local_end)),
    )
    state_entering = before_state + init_state * before_decay[:, :, None]
    query_since_beginning = query_decayed * jnp.exp(prefix_log)[:, :, None, :]
    incoming_state = jnp.einsum("oltu,luf->oltf", query_since_beginning, state_entering)
    attn = within + carried_out + incoming_state
    normal_attn = (
        attn * lax.rsqrt(jnp.mean(attn * attn, axis=-1, keepdims=True) + epsilon) * head_gain
    )
    normal_attn = normal_attn.transpose(0, 2, 1, 3).reshape(row_count, local_heads * HV)
    return (normal_attn * jax.nn.silu(out_gate.astype(F32))).astype(BF16)


def per_device(
    tokens, norm_gain, w_conv_a, w_conv_gate, conv_weight, conv_gain, w_query, w_key, w_value,
    w_outgate, w_decay, decay_bias, decay_extra, head_gain, init_state, w_out_conv, w_out_gla,
):
    proj, dec, wout = call_first(
        tokens,
        norm_gain.reshape(64, 32),
        (w_conv_a, w_conv_gate, w_query, w_key, w_value, w_outgate, w_decay, w_out_conv, w_out_gla),
    )
    conv_out = conv_branch(proj[:, 0:128], proj[:, 128:256], conv_weight, conv_gain)
    gla_out = gla_branch(
        proj[:, 512:576], proj[:, 576:640], proj[:, 256:384], proj[:, 384:512], dec[:, 0:64],
        decay_bias, decay_extra, head_gain, init_state,
    )
    out_conv = wout[:, 0:32, :].reshape(D, 128)
    out_gla = wout[:, 32:64, :].reshape(D, 128)
    partial = jnp.einsum("rk,nk->rn", conv_out, out_conv, preferred_element_type=F32) + jnp.einsum(
        "rk,nk->rn", gla_out, out_gla, preferred_element_type=F32
    )
    return lax.psum_scatter(partial.astype(BF16), TP, scatter_dimension=0, tiled=True)


def solution(mesh):
    torus = Mesh(mesh.devices.reshape(NZ, NY, NX, NC), ("z", "y", "x", "c"))
    placed = (
        P(SP, TP),
        P(),
        P(SP, TP),
        P(SP, TP),
        P(None, TP),
        P(TP),
        P(SP, TP),
        P(SP, TP),
        P(SP, TP),
        P(SP, TP),
        P(SP, TP),
        P(TP),
        P(SP, TP),
        P(),
        P(TP, None, None),
        P(TP, SP),
        P(TP, SP),
    )
    return jax.shard_map(
        per_device, mesh=torus, in_specs=placed, out_specs=P(SP_TP, None), check_vma=False
    )
```

```python
import jax
import jax.numpy as jnp
from jax import lax
from jax.experimental import pallas as pl
from jax.experimental.pallas import tpu as pltpu
from jax.sharding import Mesh
from jax.sharding import PartitionSpec as P

D = 2048
D_CONV = 1024
ROWS = 1024
TAPS = 31
NZ, NY, NX, NC = 16, 4, 4, 2
SP = ("z", "y")
TP = ("x", "c")
SP_TP = ("z", "y", "x", "c")
RA, RM, RT = 96, 176, 240
F32, BF16 = jnp.float32, jnp.bfloat16

epsilon = 1e-06
gate_divisor = 16.0


def remote(src, dst, send, recv, **ids):
    return pltpu.make_async_remote_copy(
        src_ref=src,
        dst_ref=dst,
        send_sem=send,
        recv_sem=recv,
        device_id=ids,
        device_id_type=pl.DeviceIdType.MESH,
    )


class Mover:
    def __init__(self):
        self.sent = []

    def send(self, ref, send, recv, **ids):
        copy = remote(ref, ref, send, recv, **ids)
        copy.start()
        self.sent.append(copy)

    def drain(self):
        for copy in self.sent:
            copy.wait_send()
        self.sent = []


def arrived(ref, send, recv, **ids):
    remote(ref, ref, send, recv, **ids).wait_recv()


def pack_chunk(sp, gain, wa, wg, wq, wk, wv, wo, wd, woc, wog, G):
    row = gain[pl.ds(sp // 4, 1), :]
    r = lax.broadcasted_iota(jnp.int32, (32, 128), 0)
    lane = lax.broadcasted_iota(jnp.int32, (32, 128), 1)
    mine = lane == r + 32 * lax.rem(sp, 4)
    col = jnp.sum(jnp.where(mine, jnp.broadcast_to(row, (32, 128)), 0.0), axis=1, keepdims=True)

    def scaled(ref):
        return ref[...].astype(F32) * col

    d = scaled(wd)
    G[sp, 0:32] = scaled(wv).astype(BF16)
    G[sp, 32:64] = jnp.concatenate([scaled(wq), scaled(wk)], axis=1).astype(BF16)
    G[sp, 64:96] = scaled(wa).astype(BF16)
    G[sp, 96:112] = jnp.concatenate([d[0:16], d[16:32]], axis=1).astype(BF16)
    G[sp, 112:144] = scaled(wg).astype(BF16)
    G[sp, 144:176] = scaled(wo).astype(BF16)
    G[sp, 176:208] = woc[...]
    G[sp, 208:240] = wog[...]


def greet(z, y, x, c):
    barrier = pltpu.get_barrier_semaphore()
    partners = [dict(z=lax.rem(z + d, NZ)) for d in range(1, NZ)]
    partners += [dict(y=lax.rem(y + d, NY)) for d in range(1, NY)]
    partners += [peer(x, c, r) for r in range(1, NX * NC)]
    partners += [following(z, y, 1), following(z, y, -1)]
    for ids in partners:
        pl.semaphore_signal(barrier, inc=1, device_id=ids, device_id_type=pl.DeviceIdType.MESH)
    pl.semaphore_wait(barrier, len(partners))


def peer(x, c, r):
    return dict(x=lax.rem(x + r // 2, NX), c=1 - c if r % 2 else c)


def back_peer(x, c, r):
    return dict(x=lax.rem(x + NX - r // 2, NX), c=1 - c if r % 2 else c)


def following(z, y, d):
    sp = lax.rem(z * NY + y + d + NZ * NY, NZ * NY)
    return dict(z=sp // NY, y=lax.rem(sp, NY))


def gather(z, y, x, c, tokens, G, tok, local, sems, meanwhile):
    (a1s, a1r, a2s, a2r, b1s, b1r, b2s, b2r, xs, xr, ds_, dr) = sems
    sp = z * NY + y
    zr, zl = lax.rem(z + 1, NZ), lax.rem(z + NZ - 1, NZ)
    yr, yl = lax.rem(y + 1, NY), lax.rem(y + NY - 1, NY)
    xr_, xl_ = lax.rem(x + 1, NX), lax.rem(x + NX - 1, NX)
    xo = lax.rem(x + 2, NX)
    co = 1 - c
    m = Mover()

    def slab(xi, ci, half):
        col = pl.multiple_of((xi * NC + ci) * 256, 256)
        return tok.at[pl.ds(half * 512, 512), pl.ds(col, 256)]

    def zc(s):
        return lax.rem(z + s + 2 * NZ, NZ)

    own = pltpu.make_async_copy(
        tokens, tok.at[:, pl.ds(pl.multiple_of((x * NC + c) * 256, 256), 256)], local
    )
    own.start()
    greet(z, y, x, c)

    for d in (1, 3, 2):
        m.send(G.at[sp, 0:RA], a1s.at[d - 1], a1r.at[d - 1], y=lax.rem(y + d, NY))

    def b1(s):
        if 0 <= s < 8:
            m.send(G.at[zc(-s) * NY + y, RA:RT], b1s.at[0, s], b1r.at[0, s], z=zr)
        if 0 <= s < 7:
            m.send(G.at[zc(s) * NY + y, RA:RT], b1s.at[1, s], b1r.at[1, s], z=zl)

    def b1_in(s):
        arrived(G.at[zc(-s) * NY + y, RA:RT], b1s.at[0, 0], b1r.at[0, s - 1], z=zl)
        if s <= 7:
            arrived(G.at[zc(s) * NY + y, RA:RT], b1s.at[0, 0], b1r.at[1, s - 1], z=zr)

    def both(s):
        return [(s, -s)] if s in (0, 8) else [(s, -s), (s + 8, s)]

    def b2(s):
        for k, off in both(s):
            ref = G.at[zc(off) * NY + y, RA:RT]
            m.send(ref, b2s.at[0, k], b2r.at[0, k], y=yr)
            m.send(ref, b2s.at[1, k], b2r.at[1, k], y=yl)

    def b2_forward(s):
        for k, off in both(s):
            first = zc(off) * NY
            arrived(G.at[first + yl, RA:RT], b2s.at[0, 0], b2r.at[0, k], y=yl)
            m.send(G.at[first + yl, RA:RM], b2s.at[2, k], b2r.at[2, k], y=yr)
            arrived(G.at[first + yr, RA:RT], b2s.at[0, 0], b2r.at[1, k], y=yr)
            m.send(G.at[first + yr, RM:RT], b2s.at[3, k], b2r.at[3, k], y=yl)

    def b2_end(s):
        yo = lax.rem(y + 2, NY)
        for k, off in both(s):
            first = zc(off) * NY
            arrived(G.at[first + yo, RA:RM], b2s.at[0, 0], b2r.at[2, k], y=yl)
            arrived(G.at[first + yo, RM:RT], b2s.at[0, 0], b2r.at[3, k], y=yr)

    def a2(s, p):
        if s < 8:
            m.send(G.at[pl.ds(zc(-s) * NY + 2 * p, 2), 0:RA], a2s.at[0, s, p], a2r.at[0, s, p], z=zr)
        if s < 7:
            m.send(G.at[pl.ds(zc(s) * NY + 2 * p, 2), 0:RA], a2s.at[1, s, p], a2r.at[1, s, p], z=zl)

    def a2_in(s, p):
        arrived(G.at[pl.ds(zc(-s) * NY + 2 * p, 2), 0:RA], a2s.at[0, 0, 0], a2r.at[0, s - 1, p], z=zl)
        if s <= 7:
            arrived(G.at[pl.ds(zc(s) * NY + 2 * p, 2), 0:RA], a2s.at[0, 0, 0], a2r.at[1, s - 1, p], z=zr)

    def xsend(ref, k, **ids):
        m.send(ref, xs.at[k], xr.at[k], **ids)

    def xin(ref, k, **ids):
        arrived(ref, xs.at[0], xr.at[k], **ids)

    def pair(ref, k):
        m.send(ref, ds_.at[k], dr.at[k], c=co)

    b1(0)
    own.wait()
    xsend(slab(x, c, 0), 0, x=xr_)
    xsend(slab(x, c, 1), 1, x=xl_)
    xsend(slab(x, c, 1), 2, x=xr_)
    xsend(slab(x, c, 0), 3, x=xl_)
    pair(slab(x, c, 0), 0)
    pair(slab(x, c, 1), 1)
    b2(0)
    for d in (1, 2, 3):
        arrived(G.at[z * NY + lax.rem(y + NY - d, NY), 0:RA], a1s.at[0], a1r.at[d - 1], y=lax.rem(y + NY - d, NY))
    for p in (0, 1):
        a2(0, p)
    meanwhile()
    for s in range(1, 9):
        b1_in(s)
        b1(s)
        b2(s)
        for p in (0, 1):
            a2_in(s, p)
            a2(s, p)
        b2_forward(s - 1)
        if s == 3:
            xin(slab(xl_, c, 0), 0, x=xl_)
            xsend(slab(xl_, c, 0), 4, x=xr_)
            pair(slab(xl_, c, 0), 2)
            xin(slab(xr_, c, 1), 1, x=xr_)
            xsend(slab(xr_, c, 1), 5, x=xl_)
            pair(slab(xr_, c, 1), 3)
        if s == 6:
            xin(slab(xl_, c, 1), 2, x=xl_)
            pair(slab(xl_, c, 1), 4)
            xin(slab(xr_, c, 0), 3, x=xr_)
            pair(slab(xr_, c, 0), 5)
    b2_forward(8)
    xin(slab(xo, c, 0), 4, x=xl_)
    pair(slab(xo, c, 0), 6)
    xin(slab(xo, c, 1), 5, x=xr_)
    pair(slab(xo, c, 1), 7)
    for s in range(9):
        b2_end(s)
    arrivals = [(x, 0), (x, 1), (xl_, 0), (xr_, 1), (xl_, 1), (xr_, 0), (xo, 0), (xo, 1)]
    for k, (xi, half) in enumerate(arrivals):
        arrived(slab(xi, co, half), ds_.at[0], dr.at[k], c=co)
    m.drain()


GATHER_SEMS = [
    pltpu.SemaphoreType.DMA((3,)),
    pltpu.SemaphoreType.DMA((3,)),
    pltpu.SemaphoreType.DMA((2, 8, 2)),
    pltpu.SemaphoreType.DMA((2, 8, 2)),
    pltpu.SemaphoreType.DMA((2, 8)),
    pltpu.SemaphoreType.DMA((2, 8)),
    pltpu.SemaphoreType.DMA((4, 16)),
    pltpu.SemaphoreType.DMA((4, 16)),
    pltpu.SemaphoreType.DMA((6,)),
    pltpu.SemaphoreType.DMA((6,)),
    pltpu.SemaphoreType.DMA((8,)),
    pltpu.SemaphoreType.DMA((8,)),
]


def spread_weights(G, W):
    def step(k, _):
        rows = pl.ds(pl.multiple_of(k * 256, 256), 256)
        sps = pl.ds(k * 8, 8)
        for at, first in ((0, 64), (128, 112), (256, 0), (384, 144), (512, 32)):
            W[rows, at : at + 128] = G[sps, first : first + 32, :].reshape(256, 128)
        d = G[sps, 96:112, :].astype(F32)
        both = jnp.concatenate([d[:, :, 0:64], d[:, :, 64:128]], axis=1).reshape(256, 64)
        W[rows, 640:768] = jnp.concatenate([both, both], axis=1).astype(BF16)
        return 0

    lax.fori_loop(0, 8, step, 0)


def nt(a, b):
    return lax.dot_general(a, b, (((1,), (1,)), ((), ())), preferred_element_type=F32)


def tn(a, b):
    return lax.dot_general(a, b, (((0,), (0,)), ((), ())), preferred_element_type=F32)


def nn(a, b):
    return jnp.dot(a, b, preferred_element_type=F32)


def again(x):
    return x.astype(BF16).astype(F32)


def iota(shape, axis):
    return lax.broadcasted_iota(jnp.int32, shape, axis)


def project_rows(tok, W, gext, v, og, qk, dec):
    def block(i, _):
        first = pl.multiple_of(i * 256, 256)
        rows = pl.ds(first, 256)
        t = tok[rows, :]
        acc = jnp.zeros((256, 128), F32)
        for k in range(16):
            piece = t[:, k * 128 : k * 128 + 128].astype(F32)
            acc = acc + piece * piece
        scale = lax.rsqrt(jnp.sum(acc, axis=1, keepdims=True) * (1.0 / D) + epsilon)
        part = nn(t, W[:, 0:256]) * scale
        gated = again(part[:, 0:128]) * jax.nn.sigmoid(again(part[:, 128:256]))
        gext[pl.ds(first + 32, 256), :] = again(gated)
        part = nn(t, W[:, 256:512]) * scale
        v[rows, :] = part[:, 0:128].astype(BF16)
        og[rows, :] = part[:, 128:256].astype(BF16)
        part = nn(t, W[:, 512:768]) * scale
        qk[rows, :] = again(part[:, 0:128])
        dec[rows, :] = part[:, 128:256]
        return 0

    lax.fori_loop(0, 4, block, 0)


def block_products(i, bias, extra, dec, qk, v, SQ, kv, tots):
    rows = slice(i * 256, i * 256 + 256)
    pre = dec[rows, :] + bias
    log = jnp.minimum(pre, 0.0) - jnp.log1p(jnp.exp(-jnp.abs(pre)))
    cum = log * (1.0 / gate_divisor) + extra[rows, :]
    place = lax.rem(iota((256, 128), 0), 64)
    for s in (1, 2, 4, 8, 16, 32):
        cum = cum + jnp.where(place >= s, pltpu.roll(cum, s, 0), 0.0)
    total = cum.reshape(4, 64, 128)[:, 63:64, :]
    tots[4 * i : 4 * i + 4, :] = total.reshape(4, 128)
    total = jnp.broadcast_to(total, (4, 64, 128)).reshape(256, 128)
    low = iota((256, 128), 1) < 64
    a = qk[rows, :]
    b = pltpu.roll(a, 64, 1)
    q = jnp.where(low, a, b) * 0.125
    k = jnp.where(low, b, a)
    q = q * jnp.exp(cum)
    inverse = k * jnp.exp(-cum)
    to_end = k * jnp.exp(total - cum)
    r, s = iota((256, 256), 0), iota((256, 256), 1)
    same = r // 64 == s // 64
    scores = nt(jnp.where(low, q, 0.0).astype(BF16), inverse.astype(BF16))
    SQ[rows, 0:256] = jnp.where(same & (s <= r), scores, 0.0).astype(BF16)
    SQ[rows, 256:512] = jnp.where(same, jnp.concatenate([q, q], axis=1), 0.0).astype(BF16)
    spread = jnp.where(same, jnp.concatenate([to_end, to_end], axis=1), 0.0).astype(BF16)
    kv[rows, :] = tn(spread, v[rows, :])


def conv_sums(cw, gext, csum, mine):
    for b in range(8):
        acc = jnp.zeros((128, 128), F32)
        for j in range(TAPS):
            acc = acc + cw[j : j + 1, :] * gext[128 * b + 2 + j : 128 * b + 130 + j, :]
        csum[128 * b : 128 * b + 128, :] = acc
        t = acc.T
        mine[b : b + 1, :] = jnp.sum(t, axis=0, keepdims=True)
        mine[8 + b : 9 + b, :] = jnp.sum(t * t, axis=0, keepdims=True)


def conv_finish(cst, square, csum, conv_gain, X):
    both = cst[0]
    for k in range(1, 8):
        both = both + cst[k]
    both = both * (1.0 / D_CONV)
    mean = both[0:8]
    square[0:8, :] = mean
    square[8:16, :] = lax.rsqrt(both[8:16] - mean * mean + epsilon)
    t = square[...].T
    for b in range(8):
        n = (csum[128 * b : 128 * b + 128, :] - t[:, b : b + 1]) * t[:, 8 + b : 9 + b] * conv_gain
        X[128 * b : 128 * b + 128, 0:128] = (n * jax.nn.sigmoid(n)).astype(BF16)


def layer(tokens, gain, wa, wg, cw, conv_gain, wq, wk, wv, wo, wd, bias, extra_t, head_gain, init, woc, wog,
          out, G, tok, W, gext, v, og, qk, dec, extra, SQ, kv, tots, square, csum, cst, hout, hin, ybuf, ztot,
          zbuf, fbuf, Sst, X, pout, pin, s0, s1, s2, r0, r1, fl, fr, facc,
          local, hs, hr, cs, cr, ys, yr, zs, zr, fs, fr_, ps, pr, gs, gr, *sems):
    z, y, x, c = (lax.axis_index(n) for n in ("z", "y", "x", "c"))
    sp = z * NY + y
    tp = x * NC + c
    m = Mover()
    pack_chunk(sp, gain, wa, wg, wq, wk, wv, wo, wd, woc, wog, G)
    zbuf[...] = jnp.zeros_like(zbuf)

    def meanwhile():
        for b in range(8):
            e = extra_t[:, 128 * b : 128 * b + 128]
            extra[128 * b : 128 * b + 128, :] = jnp.concatenate([e, e], axis=0).T
        tots[...] = jnp.zeros_like(tots)
        square[...] = jnp.zeros_like(square)

    gather(z, y, x, c, tokens, G, tok, local, sems, meanwhile)
    spread_weights(G, W)
    project_rows(tok, W, gext, v, og, qk, dec)

    hout[...] = gext[ROWS : ROWS + 32, :].astype(BF16)
    after, ahead = following(z, y, 1), following(z, y, -1)
    halo = remote(hout, hin, hs.at[0], hr.at[0], **after)
    halo.start()

    b2 = jnp.concatenate([bias[...], bias[...]], axis=1)
    for i in range(4):
        block_products(i, b2, extra, dec, qk, v, SQ, kv, tots)
    tt = tots[...].T[0:64, :]
    decay = jnp.exp(tt)
    state = jnp.zeros((64, 128), F32)
    for b in range(16):
        state = state * decay[:, b : b + 1] + kv[64 * b : 64 * b + 64, :]
    ybuf[y, 0:64] = state.astype(BF16)
    ybuf[y, 64:128] = jnp.broadcast_to(jnp.exp(jnp.sum(tt, axis=1, keepdims=True)), (64, 128)).astype(BF16)
    for d in (1, 3, 2):
        m.send(ybuf.at[y], ys.at[d - 1], yr.at[d - 1], y=lax.rem(y + d, NY))

    halo.wait_send()
    remote(hout, hin, hs.at[0], hr.at[0], **ahead).wait_recv()
    gext[0:32, :] = jnp.where(sp > 0, hin[...].astype(F32), 0.0)
    conv_sums(cw, gext, csum, cst.at[tp])
    for r in range(1, 8):
        m.send(cst.at[tp], cs.at[r - 1], cr.at[r - 1], **peer(x, c, r))

    for d in (1, 2, 3):
        yd = lax.rem(y + NY - d, NY)
        arrived(ybuf.at[yd], ys.at[0], yr.at[d - 1], y=yd)
    row_state = jnp.zeros((64, 128), F32)
    row_decay = jnp.ones((64, 128), F32)
    pre_state, pre_decay = row_state, row_decay
    for k in range(NY):
        pre_state = jnp.where(y == k, row_state, pre_state)
        pre_decay = jnp.where(y == k, row_decay, pre_decay)
        a = ybuf[k, 64:128].astype(F32)
        row_state = row_state * a + ybuf[k, 0:64].astype(F32)
        row_decay = row_decay * a
    ztot[0] = row_state
    ztot[1] = row_decay
    ztot[2] = pre_state
    ztot[3] = pre_decay
    part = pl.ds(pl.multiple_of(y * 16, 16), 16)
    zbuf[z, 0:16] = ztot[0, part, :].astype(BF16)
    zbuf[z, 16:32] = ztot[1, part, :].astype(BF16)
    for d in range(1, NZ):
        @pl.when(z + d < NZ)
        def _():
            remote(zbuf.at[z], zbuf.at[z], zs.at[d - 1], zr.at[d - 1], z=lax.rem(z + d, NZ)).start()

    for r in range(1, 8):
        ids = back_peer(x, c, r)
        arrived(cst.at[ids["x"] * NC + ids["c"]], cs.at[0], cr.at[r - 1], **ids)
    conv_finish(cst, square, csum, conv_gain[...], X)

    for d in range(1, NZ):
        @pl.when(z >= d)
        def _():
            zd = lax.rem(z + NZ - d, NZ)
            arrived(zbuf.at[zd], zs.at[0], zr.at[d - 1], z=zd)
    state = init[part, :]
    for k in range(NZ - 1):
        following_state = state * zbuf[k, 16:32].astype(F32) + zbuf[k, 0:16].astype(F32)
        state = jnp.where(k < z, following_state, state)
    fbuf[y] = state.astype(BF16)
    for d in (1, 3, 2):
        m.send(fbuf.at[y], fs.at[d - 1], fr_.at[d - 1], y=lax.rem(y + d, NY))
    for d in (1, 2, 3):
        yd = lax.rem(y + NY - d, NY)
        arrived(fbuf.at[yd], fs.at[0], fr_.at[d - 1], y=yd)
    state = fbuf[...].reshape(64, 128).astype(F32) * ztot[3] + ztot[2]
    for b in range(16):
        Sst[64 * b : 64 * b + 64, :] = state.astype(BF16)
        state = state * decay[:, b : b + 1] + kv[64 * b : 64 * b + 64, :]
    for i in range(4):
        rows = slice(256 * i, 256 * i + 256)
        attn = nn(SQ[rows, 0:256], v[rows, :]) + nn(SQ[rows, 256:512], Sst[rows, :])
        mean = jnp.sum(attn * attn, axis=1, keepdims=True) * (1.0 / 128.0)
        o = og[rows, :].astype(F32)
        X[rows, 128:256] = (
            attn * lax.rsqrt(mean + epsilon) * head_gain[...] * (o * jax.nn.sigmoid(o))
        ).astype(BF16)

    xr, xl, xo = lax.rem(x + 1, NX), lax.rem(x + NX - 1, NX), lax.rem(x + 2, NX)
    order = (xo, xr, xl, x)

    def product(xi, ci, n):
        rows = pl.ds(pl.multiple_of((xi * NC + ci) * 128, 128), 128)
        w = jnp.concatenate(
            [
                G[16 * n : 16 * n + 16, 176:208, :].reshape(512, 128),
                G[16 * n : 16 * n + 16, 208:240, :].reshape(512, 128),
            ],
            axis=1,
        )
        return nt(X[rows, :], w)

    def for_pair(q):
        for n in range(4):
            pout[q, :, 512 * n : 512 * n + 512] = product(order[q], 1 - c, n).astype(BF16)
        copy = remote(pout.at[q], pin.at[q], ps.at[q], pr.at[q], c=1 - c)
        copy.start()
        m.sent.append(copy)

    def pair_sum(q, to):
        remote(pout.at[q], pin.at[q], ps.at[q], pr.at[q], c=1 - c).wait_recv()
        for n in range(4):
            cols = slice(512 * n, 512 * n + 512)
            to[:, cols] = (product(order[q], c, n) + pin[q, :, cols].astype(F32)).astype(to.dtype)

    def ring(k, src, dst, xi):
        copy = remote(src, dst, gs.at[k], gr.at[k], x=xi)
        copy.start()
        m.sent.append(copy)

    def ring_in(k, dst, xi):
        remote(dst, dst, gs.at[k], gr.at[k], x=xi).wait_recv()

    top, low = pl.ds(0, 64), pl.ds(64, 64)
    for_pair(0)
    for_pair(1)
    pair_sum(0, s0)
    ring(0, s0.at[top], r0, xr)
    ring(1, s0.at[low], r1, xl)
    for_pair(2)
    pair_sum(1, s1)
    ring(2, s1.at[low], fl.at[low], xr)
    pair_sum(2, s2)
    ring(3, s2.at[top], fr.at[top], xl)
    for_pair(3)
    pair_sum(3, facc)
    ring_in(0, r0, xl)
    s1[0:64, :] = (s1[0:64, :].astype(F32) + r0[...].astype(F32)).astype(BF16)
    ring(4, s1.at[top], fl.at[top], xr)
    ring_in(1, r1, xr)
    s2[64:128, :] = (s2[64:128, :].astype(F32) + r1[...].astype(F32)).astype(BF16)
    ring(5, s2.at[low], fr.at[low], xl)
    ring_in(2, fl.at[low], xl)
    ring_in(3, fr.at[top], xr)
    ring_in(4, fl.at[top], xl)
    out[0:64, :] = (facc[0:64, :] + fl[0:64, :].astype(F32) + fr[0:64, :].astype(F32)).astype(BF16)
    ring_in(5, fr.at[low], xr)
    out[64:128, :] = (facc[64:128, :] + fl[64:128, :].astype(F32) + fr[64:128, :].astype(F32)).astype(BF16)
    m.drain()
    for d in range(1, NZ):
        @pl.when(z + d < NZ)
        def _():
            remote(zbuf.at[z], zbuf.at[z], zs.at[d - 1], zr.at[d - 1], z=lax.rem(z + d, NZ)).wait_send()


def per_device(
    tokens, norm_gain, w_conv_a, w_conv_gate, conv_weight, conv_gain, w_query, w_key, w_value,
    w_outgate, w_decay, decay_bias, decay_extra, head_gain, init_state, w_out_conv, w_out_gla,
):
    vm = pl.BlockSpec(memory_space=pltpu.VMEM)
    dma = pltpu.SemaphoreType.DMA
    scratch = [
        pltpu.VMEM((64, RT, 128), BF16),
        pltpu.VMEM((ROWS, D), BF16),
        pltpu.VMEM((D, 768), BF16),
        pltpu.VMEM((ROWS + 32, 128), F32),
        pltpu.VMEM((ROWS, 128), BF16),
        pltpu.VMEM((ROWS, 128), BF16),
        pltpu.VMEM((ROWS, 128), F32),
        pltpu.VMEM((ROWS, 128), F32),
        pltpu.VMEM((ROWS, 128), F32),
        pltpu.VMEM((ROWS, 512), BF16),
        pltpu.VMEM((ROWS, 128), F32),
        pltpu.VMEM((128, 128), F32),
        pltpu.VMEM((128, 128), F32),
        pltpu.VMEM((ROWS, 128), F32),
        pltpu.VMEM((8, 16, 128), F32),
        pltpu.VMEM((32, 128), BF16),
        pltpu.VMEM((32, 128), BF16),
        pltpu.VMEM((NY, 128, 128), BF16),
        pltpu.VMEM((4, 64, 128), F32),
        pltpu.VMEM((NZ, 32, 128), BF16),
        pltpu.VMEM((NY, 16, 128), BF16),
        pltpu.VMEM((ROWS, 128), BF16),
        pltpu.VMEM((ROWS, 256), BF16),
        pltpu.VMEM((4, 128, D), BF16),
        pltpu.VMEM((4, 128, D), BF16),
        pltpu.VMEM((128, D), BF16),
        pltpu.VMEM((128, D), BF16),
        pltpu.VMEM((128, D), BF16),
        pltpu.VMEM((64, D), BF16),
        pltpu.VMEM((64, D), BF16),
        pltpu.VMEM((128, D), BF16),
        pltpu.VMEM((128, D), BF16),
        pltpu.VMEM((128, D), F32),
        dma,
    ] + [dma((n,)) for n in (1, 1, 7, 7, 3, 3, 15, 15, 3, 3, 4, 4, 6, 6)]
    return pl.pallas_call(
        layer,
        out_shape=jax.ShapeDtypeStruct((128, D), BF16),
        in_specs=[pl.BlockSpec(memory_space=pl.ANY)] + [vm] * 16,
        out_specs=vm,
        scratch_shapes=scratch + GATHER_SEMS,
        compiler_params=pltpu.CompilerParams(
            collective_id=0, has_side_effects=True, vmem_limit_bytes=60 * 1024 * 1024
        ),
    )(
        tokens, norm_gain.reshape(16, 128), w_conv_a, w_conv_gate, conv_weight, conv_gain.reshape(1, 128),
        w_query, w_key, w_value, w_outgate, w_decay, decay_bias.reshape(1, 64), decay_extra.T,
        head_gain.reshape(1, 128), init_state.reshape(64, 128), w_out_conv.T, w_out_gla.T,
    )


def solution(mesh):
    torus = Mesh(mesh.devices.reshape(NZ, NY, NX, NC), ("z", "y", "x", "c"))
    placed = (
        P(SP, TP),
        P(),
        P(SP, TP),
        P(SP, TP),
        P(None, TP),
        P(TP),
        P(SP, TP),
        P(SP, TP),
        P(SP, TP),
        P(SP, TP),
        P(SP, TP),
        P(TP),
        P(SP, TP),
        P(),
        P(TP, None, None),
        P(TP, SP),
        P(TP, SP),
    )
    return jax.shard_map(
        per_device, mesh=torus, in_specs=placed, out_specs=P(SP_TP, None), check_vma=False
    )
```

```python
import jax
import jax.numpy as jnp
from jax import lax
from jax.experimental import pallas as pl
from jax.experimental.pallas import tpu as pltpu
from jax.sharding import Mesh
from jax.sharding import PartitionSpec as P

D = 2048
D_CONV = 1024
ROWS = 1024
TAPS = 31
NZ, NY, NX, NC = 16, 4, 4, 2
SP = ("z", "y")
TP = ("x", "c")
SP_TP = ("z", "y", "x", "c")
PARTS = ((0, 80), (80, 176), (176, 240))
PAIRS = ((0,), (1, 2), (3, 4), (5, 6), (7, 8))
F32, BF16 = jnp.float32, jnp.bfloat16

epsilon = 1e-06
gate_divisor = 16.0


def remote(src, dst, send, recv, **ids):
    return pltpu.make_async_remote_copy(
        src_ref=src,
        dst_ref=dst,
        send_sem=send,
        recv_sem=recv,
        device_id=ids,
        device_id_type=pl.DeviceIdType.MESH,
    )


class Mover:
    def __init__(self):
        self.sent = []

    def send(self, ref, send, recv, **ids):
        copy = remote(ref, ref, send, recv, **ids)
        copy.start()
        self.sent.append(copy)

    def drain(self):
        for copy in self.sent:
            copy.wait_send()
        self.sent = []


def arrived(ref, send, recv, **ids):
    remote(ref, ref, send, recv, **ids).wait_recv()


def pack_chunk(sp, gain, wa, wg, wq, wk, wv, wo, wd, woc, wog, G):
    row = gain[pl.ds(sp // 4, 1), :]
    r = lax.broadcasted_iota(jnp.int32, (32, 128), 0)
    lane = lax.broadcasted_iota(jnp.int32, (32, 128), 1)
    mine = lane == r + 32 * lax.rem(sp, 4)
    col = jnp.sum(jnp.where(mine, jnp.broadcast_to(row, (32, 128)), 0.0), axis=1, keepdims=True)

    def scaled(ref):
        return ref[...].astype(F32) * col

    d = scaled(wd)
    G[sp, 0:32] = scaled(wv).astype(BF16)
    G[sp, 32:64] = jnp.concatenate([scaled(wq), scaled(wk)], axis=1).astype(BF16)
    G[sp, 64:80] = jnp.concatenate([d[0:16], d[16:32]], axis=1).astype(BF16)
    G[sp, 80:112] = scaled(wa).astype(BF16)
    G[sp, 112:144] = scaled(wg).astype(BF16)
    G[sp, 144:176] = scaled(wo).astype(BF16)
    G[sp, 176:208] = woc[...]
    G[sp, 208:240] = wog[...]


def greet(z, y, x, c):
    barrier = pltpu.get_barrier_semaphore()
    partners = [dict(z=lax.rem(z + d, NZ)) for d in (1, 2, NZ - 2, NZ - 1)]
    partners += [dict(y=lax.rem(y + d, NY)) for d in range(1, NY)]
    partners += [peer(x, c, r) for r in range(1, NX * NC)]
    partners += [following(z, y, 1), following(z, y, -1)]
    for ids in partners:
        pl.semaphore_signal(barrier, inc=1, device_id=ids, device_id_type=pl.DeviceIdType.MESH)
    pl.semaphore_wait(barrier, len(partners))


def peer(x, c, r):
    return dict(x=lax.rem(x + r // 2, NX), c=1 - c if r % 2 else c)


def back_peer(x, c, r):
    return dict(x=lax.rem(x + NX - r // 2, NX), c=1 - c if r % 2 else c)


def following(z, y, d):
    sp = lax.rem(z * NY + y + d + NZ * NY, NZ * NY)
    return dict(z=sp // NY, y=lax.rem(sp, NY))


class Weights:
    def __init__(self, m, z, y, G, zs, zr, ys, yr):
        self.m, self.z, self.y, self.G = m, z, y, G
        self.zs, self.zr, self.ys, self.yr = zs, zr, ys, yr
        self.up, self.down, self.over = (lax.rem(y + d, NY) for d in (1, 3, 2))

    def chunk(self, o, y, first, last):
        return self.G.at[lax.rem(self.z - o + NZ, NZ) * NY + y, first:last]

    def cuts(self, p, o):
        first, last = PARTS[p]
        return first, first + (48, 32)[o % 2] if p == 0 else (first + last) // 2, last

    def z_out(self, p, o):
        step = (2 if abs(o) > 1 else 1) * (1 if o > 0 else -1)
        self.m.send(
            self.chunk(o - step, self.y, *PARTS[p]), self.zs.at[p, o + 7], self.zr.at[p, o + 7], z=lax.rem(self.z + step + NZ, NZ)
        )

    def y_out(self, p, o):
        for k, to in enumerate((self.up, self.down)):
            self.m.send(self.chunk(o, self.y, *PARTS[p]), self.ys.at[p, o + 7, k], self.yr.at[p, o + 7, k], y=to)

    def begin(self, p):
        for o in (1, -1, 2, -2):
            self.z_out(p, o)
        self.y_out(p, 0)

    def offsets(self, pair):
        return [o for a in pair for o in ((a, -a) if a not in (0, 8) else (a,))]

    def relay(self, p, pair):
        for o in self.offsets(pair):
            arrived(self.chunk(o, self.y, *PARTS[p]), self.zs.at[p, 7], self.zr.at[p, o + 7], z=lax.rem(self.z + 1, NZ))
            further = o + 2 if o > 0 else o - 2
            if -7 <= further <= 8:
                self.z_out(p, further)
            self.y_out(p, o)

    def forward(self, p, pair):
        for o in self.offsets(pair):
            first, middle, last = self.cuts(p, o)
            arrived(self.chunk(o, self.down, first, last), self.ys.at[p, 0, 0], self.yr.at[p, o + 7, 0], y=self.down)
            self.m.send(self.chunk(o, self.down, first, middle), self.ys.at[p, o + 7, 2], self.yr.at[p, o + 7, 2], y=self.up)
            arrived(self.chunk(o, self.up, first, last), self.ys.at[p, 0, 0], self.yr.at[p, o + 7, 1], y=self.up)
            self.m.send(self.chunk(o, self.up, middle, last), self.ys.at[p, o + 7, 3], self.yr.at[p, o + 7, 3], y=self.down)

    def end(self, p):
        for pair in PAIRS:
            for o in self.offsets(pair):
                first, middle, last = self.cuts(p, o)
                arrived(self.chunk(o, self.over, first, middle), self.ys.at[p, 0, 0], self.yr.at[p, o + 7, 2], y=self.down)
                arrived(self.chunk(o, self.over, middle, last), self.ys.at[p, 0, 0], self.yr.at[p, o + 7, 3], y=self.up)


class Tokens:
    def __init__(self, m, x, c, tok, ssq, xs, xr, ds, dr):
        self.m, self.c, self.tok, self.ssq = m, c, tok, ssq
        self.xs, self.xr, self.ds, self.dr = xs, xr, ds, dr
        self.x, self.right, self.left, self.over = (lax.rem(x + d, NX) for d in (0, 1, 3, 2))
        self.order = [
            (self.x, 0), (self.x, 1), (self.left, 0), (self.right, 1),
            (self.left, 1), (self.right, 0), (self.over, 0), (self.over, 1),
        ]

    def slab(self, xi, ci, half):
        col = pl.multiple_of((xi * NC + ci) * 256, 256)
        return self.tok.at[pl.ds(half * 512, 512), pl.ds(col, 256)]

    def send(self, xi, half, k, to):
        self.m.send(self.slab(xi, self.c, half), self.xs.at[k], self.xr.at[k], x=to)

    def begin(self):
        self.send(self.x, 0, 0, self.right)
        self.send(self.x, 1, 1, self.left)
        self.send(self.x, 1, 2, self.right)
        self.send(self.x, 0, 3, self.left)
        self.across(0)
        self.across(1)

    def across(self, k):
        self.m.send(self.slab(self.order[k][0], self.c, self.order[k][1]), self.ds.at[k], self.dr.at[k], c=1 - self.c)

    def take(self, k):
        xi, half = self.order[k]
        arrived(self.slab(xi, self.c, half), self.xs.at[0], self.xr.at[k - 2], x=self.right if k % 2 else self.left)
        if k == 2:
            self.send(xi, half, 4, self.right)
        if k == 3:
            self.send(xi, half, 5, self.left)
        self.across(k)

    def take_across(self, k):
        xi, half = self.order[k]
        arrived(self.slab(xi, 1 - self.c, half), self.ds.at[0], self.dr.at[k], c=1 - self.c)

    def squares(self, k, ci):
        xi, half = self.order[k]
        rows = slice(half * 512, half * 512 + 512)
        t = self.slab(xi, ci, half)[...].astype(F32)
        self.ssq[rows, :] += t[:, 0:128] * t[:, 0:128] + t[:, 128:256] * t[:, 128:256]


def unpack_decay(G, Wd):
    def step(k, _):
        rows = pl.ds(pl.multiple_of(k * 256, 256), 256)
        d = G[pl.ds(k * 8, 8), 64:80, :].astype(F32)
        both = jnp.concatenate([d[:, :, 0:64], d[:, :, 64:128]], axis=1).reshape(256, 64)
        Wd[rows, :] = jnp.concatenate([both, both], axis=1).astype(BF16)
        return 0

    lax.fori_loop(0, 8, step, 0)


def column(G, first):
    return G[:, first : first + 32, :].reshape(D, 128)


def nt(a, b):
    return lax.dot_general(a, b, (((1,), (1,)), ((), ())), preferred_element_type=F32)


def tn(a, b):
    return lax.dot_general(a, b, (((0,), (0,)), ((), ())), preferred_element_type=F32)


def nn(a, b):
    return jnp.dot(a, b, preferred_element_type=F32)


def again(x):
    return x.astype(BF16).astype(F32)


def iota(shape, axis):
    return lax.broadcasted_iota(jnp.int32, shape, axis)


def project_first(i, tok, G, Wd, ssq, v, qk, dec):
    rows = slice(256 * i, 256 * i + 256)
    t = tok[rows, :]
    scale = lax.rsqrt(jnp.sum(ssq[rows, :], axis=1, keepdims=True) * (1.0 / D) + epsilon)
    ssq[rows, :] = jnp.broadcast_to(scale, (256, 128))
    part = nn(t, jnp.concatenate([column(G, 0), column(G, 32)], axis=1)) * scale
    v[rows, :] = part[:, 0:128].astype(BF16)
    qk[rows, :] = again(part[:, 128:256])
    dec[rows, :] = nn(t, Wd[...]) * scale


def project_second(i, tok, G, ssq, gext, og):
    rows = slice(256 * i, 256 * i + 256)
    t = tok[rows, :]
    scale = ssq[rows, :]
    part = nn(t, jnp.concatenate([column(G, 80), column(G, 112)], axis=1))
    gated = again(part[:, 0:128] * scale) * jax.nn.sigmoid(again(part[:, 128:256] * scale))
    gext[256 * i + 32 : 256 * i + 288, :] = again(gated)
    og[rows, :] = (nn(t, column(G, 144)) * scale).astype(BF16)


def split_heads(qk, rows):
    low = iota((256, 128), 1) < 64
    a = qk[rows, :]
    b = pltpu.roll(a, 64, 1)
    return low, jnp.where(low, a, b) * 0.125, jnp.where(low, b, a)


def same_block():
    r, s = iota((256, 256), 0), iota((256, 256), 1)
    return r // 64 == s // 64, s <= r


def block_states(i, bias, extra, dec, qk, v, kv, tots):
    rows = slice(i * 256, i * 256 + 256)
    pre = dec[rows, :] + bias
    log = jnp.minimum(pre, 0.0) - jnp.log1p(jnp.exp(-jnp.abs(pre)))
    cum = log * (1.0 / gate_divisor) + extra[rows, :]
    place = lax.rem(iota((256, 128), 0), 64)
    for s in (1, 2, 4, 8, 16, 32):
        cum = cum + jnp.where(place >= s, pltpu.roll(cum, s, 0), 0.0)
    dec[rows, :] = cum
    total = cum.reshape(4, 64, 128)[:, 63:64, :]
    tots[4 * i : 4 * i + 4, :] = total.reshape(4, 128)
    total = jnp.broadcast_to(total, (4, 64, 128)).reshape(256, 128)
    _, _, k = split_heads(qk, rows)
    to_end = k * jnp.exp(total - cum)
    same, _ = same_block()
    spread = jnp.where(same, jnp.concatenate([to_end, to_end], axis=1), 0.0).astype(BF16)
    kv[rows, :] = tn(spread, v[rows, :])


def block_scores(i, dec, qk, v, Q, within):
    rows = slice(i * 256, i * 256 + 256)
    cum = dec[rows, :]
    low, q, k = split_heads(qk, rows)
    q = q * jnp.exp(cum)
    inverse = k * jnp.exp(-cum)
    same, causal = same_block()
    scores = nt(jnp.where(low, q, 0.0).astype(BF16), inverse.astype(BF16))
    scores = jnp.where(same & causal, scores, 0.0).astype(BF16)
    Q[rows, :] = jnp.where(same, jnp.concatenate([q, q], axis=1), 0.0).astype(BF16)
    within[rows, :] = nn(scores, v[rows, :])


def conv_sums(cw, gext, csum, mine):
    for b in range(8):
        acc = jnp.zeros((128, 128), F32)
        for j in range(TAPS):
            acc = acc + cw[j : j + 1, :] * gext[128 * b + 2 + j : 128 * b + 130 + j, :]
        csum[128 * b : 128 * b + 128, :] = acc
        t = acc.T
        mine[b : b + 1, :] = jnp.sum(t, axis=0, keepdims=True)
        mine[8 + b : 9 + b, :] = jnp.sum(t * t, axis=0, keepdims=True)


def conv_finish(cst, square, csum, conv_gain, X):
    both = cst[0]
    for k in range(1, 8):
        both = both + cst[k]
    both = both * (1.0 / D_CONV)
    mean = both[0:8]
    square[0:8, :] = mean
    square[8:16, :] = lax.rsqrt(both[8:16] - mean * mean + epsilon)
    t = square[...].T
    for b in range(8):
        n = (csum[128 * b : 128 * b + 128, :] - t[:, b : b + 1]) * t[:, 8 + b : 9 + b] * conv_gain
        X[128 * b : 128 * b + 128, 0:128] = (n * jax.nn.sigmoid(n)).astype(BF16)


def layer(tokens, gain, wa, wg, cw, conv_gain, wq, wk, wv, wo, wd, bias, extra_t, head_gain, init, woc, wog,
          out, G, tok, Wd, ssq, gext, v, og, qk, dec, extra, Q, within, kv, tots, square, csum, cst, hout, hin, ybuf,
          ztot, zbuf, fbuf, Sst, X, pout, pin, s0, s1, s2, r0, r1, fl, fr, facc,
          local, hs, hr, cs, cr, ys, yr, zs, zr, fs, fr_, ps, pr, gs, gr, xs, xr_, ds, dr, wzs, wzr, wys, wyr):
    z, y, x, c = (lax.axis_index(n) for n in ("z", "y", "x", "c"))
    sp = z * NY + y
    tp = x * NC + c
    m = Mover()
    t = Tokens(m, x, c, tok, ssq, xs, xr_, ds, dr)
    w = Weights(m, z, y, G, wzs, wzr, wys, wyr)
    own = pltpu.make_async_copy(tokens, tok.at[:, pl.ds(pl.multiple_of(tp * 256, 256), 256)], local)
    own.start()
    pack_chunk(sp, gain, wa, wg, wq, wk, wv, wo, wd, woc, wog, G)
    zbuf[...] = jnp.zeros_like(zbuf)
    greet(z, y, x, c)

    w.begin(0)
    own.wait()
    t.begin()
    w.begin(1)
    for b in range(8):
        e = extra_t[:, 128 * b : 128 * b + 128]
        extra[128 * b : 128 * b + 128, :] = jnp.concatenate([e, e], axis=0).T
    tots[...] = jnp.zeros_like(tots)
    square[...] = jnp.zeros_like(square)
    ssq[...] = jnp.zeros_like(ssq)
    t.squares(0, c)
    t.squares(1, c)
    w.relay(0, PAIRS[1])
    w.forward(0, PAIRS[0])
    w.relay(1, PAIRS[1])
    w.relay(0, PAIRS[2])
    w.forward(0, PAIRS[1])
    t.take(2)
    t.take(3)
    w.relay(1, PAIRS[2])
    w.forward(1, PAIRS[0])
    for k in (0, 1):
        t.take_across(k)
        t.squares(k, 1 - c)
    w.relay(0, PAIRS[3])
    w.forward(0, PAIRS[2])
    w.relay(1, PAIRS[3])
    w.forward(1, PAIRS[1])
    w.relay(0, PAIRS[4])
    w.forward(0, PAIRS[3])
    t.take(4)
    t.take(5)
    w.relay(1, PAIRS[4])
    w.begin(2)
    for k in (2, 3):
        t.squares(k, c)
        t.take_across(k)
        t.squares(k, 1 - c)
    w.forward(0, PAIRS[4])
    w.forward(1, PAIRS[2])
    for k in (4, 5):
        t.squares(k, c)
        t.take_across(k)
        t.squares(k, 1 - c)
    t.take(6)
    t.take(7)
    w.end(0)
    unpack_decay(G, Wd)
    for k in (6, 7):
        t.squares(k, c)
        t.take_across(k)
        t.squares(k, 1 - c)

    for i in range(4):
        project_first(i, tok, G, Wd, ssq, v, qk, dec)
        if i == 0:
            w.relay(2, PAIRS[1])
        if i == 2:
            w.forward(1, PAIRS[3])
    b2 = jnp.concatenate([bias[...], bias[...]], axis=1)
    for i in range(4):
        block_states(i, b2, extra, dec, qk, v, kv, tots)
        if i == 1:
            w.relay(2, PAIRS[2])
    tt = tots[...].T[0:64, :]
    decay = jnp.exp(tt)
    state = jnp.zeros((64, 128), F32)
    for b in range(16):
        state = state * decay[:, b : b + 1] + kv[64 * b : 64 * b + 64, :]
    ybuf[y, 0:64] = state.astype(BF16)
    ybuf[y, 64:128] = jnp.broadcast_to(jnp.exp(jnp.sum(tt, axis=1, keepdims=True)), (64, 128)).astype(BF16)
    for d in (1, 3, 2):
        m.send(ybuf.at[y], ys.at[d - 1], yr.at[d - 1], y=lax.rem(y + d, NY))
    w.forward(1, PAIRS[4])
    w.relay(2, PAIRS[3])
    w.end(1)

    for i in range(4):
        project_second(i, tok, G, ssq, gext, og)
        if i == 2:
            w.relay(2, PAIRS[4])
    hout[...] = gext[ROWS : ROWS + 32, :].astype(BF16)
    after, ahead = following(z, y, 1), following(z, y, -1)
    halo = remote(hout, hin, hs.at[0], hr.at[0], **after)
    halo.start()

    for d in (1, 2, 3):
        yd = lax.rem(y + NY - d, NY)
        arrived(ybuf.at[yd], ys.at[0], yr.at[d - 1], y=yd)
    row_state = jnp.zeros((64, 128), F32)
    row_decay = jnp.ones((64, 128), F32)
    pre_state, pre_decay = row_state, row_decay
    for k in range(NY):
        pre_state = jnp.where(y == k, row_state, pre_state)
        pre_decay = jnp.where(y == k, row_decay, pre_decay)
        a = ybuf[k, 64:128].astype(F32)
        row_state = row_state * a + ybuf[k, 0:64].astype(F32)
        row_decay = row_decay * a
    ztot[0] = row_state
    ztot[1] = row_decay
    ztot[2] = pre_state
    ztot[3] = pre_decay
    part = pl.ds(pl.multiple_of(y * 16, 16), 16)
    zbuf[z, 0:16] = ztot[0, part, :].astype(BF16)
    zbuf[z, 16:32] = ztot[1, part, :].astype(BF16)
    for d in range(NZ - 1, 0, -1):
        @pl.when(z + d < NZ)
        def _():
            remote(zbuf.at[z], zbuf.at[z], zs.at[d - 1], zr.at[d - 1], z=lax.rem(z + d, NZ)).start()

    block_scores(0, dec, qk, v, Q, within)
    w.forward(2, PAIRS[0])
    w.forward(2, PAIRS[1])
    halo.wait_send()
    remote(hout, hin, hs.at[0], hr.at[0], **ahead).wait_recv()
    gext[0:32, :] = jnp.where(sp > 0, hin[...].astype(F32), 0.0)
    conv_sums(cw, gext, csum, cst.at[tp])
    for r in range(1, 8):
        m.send(cst.at[tp], cs.at[r - 1], cr.at[r - 1], **peer(x, c, r))
    w.forward(2, PAIRS[2])
    for i in range(1, 4):
        block_scores(i, dec, qk, v, Q, within)
    w.forward(2, PAIRS[3])

    for r in range(1, 8):
        ids = back_peer(x, c, r)
        arrived(cst.at[ids["x"] * NC + ids["c"]], cs.at[0], cr.at[r - 1], **ids)
    conv_finish(cst, square, csum, conv_gain[...], X)

    for d in range(1, NZ):
        @pl.when(z >= d)
        def _():
            zd = lax.rem(z + NZ - d, NZ)
            arrived(zbuf.at[zd], zs.at[0], zr.at[d - 1], z=zd)
    state = init[part, :]
    for k in range(NZ - 1):
        following_state = state * zbuf[k, 16:32].astype(F32) + zbuf[k, 0:16].astype(F32)
        state = jnp.where(k < z, following_state, state)
    fbuf[y] = state.astype(BF16)
    for d in (1, 3, 2):
        m.send(fbuf.at[y], fs.at[d - 1], fr_.at[d - 1], y=lax.rem(y + d, NY))
    w.forward(2, PAIRS[4])
    for d in (1, 2, 3):
        yd = lax.rem(y + NY - d, NY)
        arrived(fbuf.at[yd], fs.at[0], fr_.at[d - 1], y=yd)
    state = fbuf[...].reshape(64, 128).astype(F32) * ztot[3] + ztot[2]
    for b in range(16):
        Sst[64 * b : 64 * b + 64, :] = state.astype(BF16)
        state = state * decay[:, b : b + 1] + kv[64 * b : 64 * b + 64, :]
    for i in range(4):
        rows = slice(256 * i, 256 * i + 256)
        attn = within[rows, :] + nn(Q[rows, :], Sst[rows, :])
        mean = jnp.sum(attn * attn, axis=1, keepdims=True) * (1.0 / 128.0)
        o = og[rows, :].astype(F32)
        X[rows, 128:256] = (
            attn * lax.rsqrt(mean + epsilon) * head_gain[...] * (o * jax.nn.sigmoid(o))
        ).astype(BF16)
    w.end(2)

    right, left, over = lax.rem(x + 1, NX), lax.rem(x + NX - 1, NX), lax.rem(x + 2, NX)
    order = (over, right, left, x)

    def product(xi, ci, n):
        rows = pl.ds(pl.multiple_of((xi * NC + ci) * 128, 128), 128)
        cols = slice(16 * n, 16 * n + 16)
        wt = jnp.concatenate([G[cols, 176:208, :].reshape(512, 128), G[cols, 208:240, :].reshape(512, 128)], axis=1)
        return nt(X[rows, :], wt)

    def half(h):
        return slice(1024 * h, 1024 * h + 1024)

    def pair(q, h):
        return remote(pout.at[q, :, half(h)], pin.at[q, :, half(h)], ps.at[q, h], pr.at[q, h], c=1 - c)

    def for_pair(q, h):
        for n in (2 * h, 2 * h + 1):
            pout[q, :, 512 * n : 512 * n + 512] = product(order[q], 1 - c, n).astype(BF16)
        copy = pair(q, h)
        copy.start()
        m.sent.append(copy)

    def pair_sum(q, h, to):
        mine = [product(order[q], c, n) for n in (2 * h, 2 * h + 1)]
        pair(q, h).wait_recv()
        for n, value in zip((2 * h, 2 * h + 1), mine):
            cols = slice(512 * n, 512 * n + 512)
            to[:, cols] = (value + pin[q, :, cols].astype(F32)).astype(to.dtype)

    def ring(k, src, dst, xi):
        copy = remote(src, dst, gs.at[k], gr.at[k], x=xi)
        copy.start()
        m.sent.append(copy)

    def ring_in(k, dst, xi):
        remote(dst, dst, gs.at[k], gr.at[k], x=xi).wait_recv()

    for_pair(0, 0)
    for_pair(0, 1)
    for_pair(1, 1)
    pair_sum(0, 0, s0)
    ring(0, s0.at[:, half(0)], r0, right)
    pair_sum(0, 1, s0)
    ring(1, s0.at[:, half(1)], r1, left)
    for_pair(2, 0)
    pair_sum(1, 1, s1)
    ring(2, s1.at[:, half(1)], fl.at[:, half(1)], right)
    for_pair(1, 0)
    pair_sum(2, 0, s2)
    ring(3, s2.at[:, half(0)], fr.at[:, half(0)], left)
    for_pair(2, 1)
    pair_sum(1, 0, s1)
    for_pair(3, 0)
    pair_sum(2, 1, s2)
    for_pair(3, 1)
    pair_sum(3, 0, facc)
    pair_sum(3, 1, facc)
    ring_in(0, r0, left)
    s1[:, half(0)] = (s1[:, half(0)].astype(F32) + r0[...].astype(F32)).astype(BF16)
    ring(4, s1.at[:, half(0)], fl.at[:, half(0)], right)
    ring_in(1, r1, right)
    s2[:, half(1)] = (s2[:, half(1)].astype(F32) + r1[...].astype(F32)).astype(BF16)
    ring(5, s2.at[:, half(1)], fr.at[:, half(1)], left)
    ring_in(2, fl.at[:, half(1)], left)
    ring_in(3, fr.at[:, half(0)], right)
    facc[:, half(0)] += fr[:, half(0)].astype(F32)
    facc[:, half(1)] += fl[:, half(1)].astype(F32)
    ring_in(4, fl.at[:, half(0)], left)
    out[:, half(0)] = (facc[:, half(0)] + fl[:, half(0)].astype(F32)).astype(BF16)
    ring_in(5, fr.at[:, half(1)], right)
    out[:, half(1)] = (facc[:, half(1)] + fr[:, half(1)].astype(F32)).astype(BF16)
    m.drain()
    for d in range(1, NZ):
        @pl.when(z + d < NZ)
        def _():
            remote(zbuf.at[z], zbuf.at[z], zs.at[d - 1], zr.at[d - 1], z=lax.rem(z + d, NZ)).wait_send()


def per_device(
    tokens, norm_gain, w_conv_a, w_conv_gate, conv_weight, conv_gain, w_query, w_key, w_value,
    w_outgate, w_decay, decay_bias, decay_extra, head_gain, init_state, w_out_conv, w_out_gla,
):
    vm = pl.BlockSpec(memory_space=pltpu.VMEM)
    dma = pltpu.SemaphoreType.DMA
    shapes = [
        ((64, 240, 128), BF16), ((ROWS, D), BF16), ((D, 128), BF16), ((ROWS, 128), F32), ((ROWS + 32, 128), F32),
        ((ROWS, 128), BF16), ((ROWS, 128), BF16), ((ROWS, 128), F32), ((ROWS, 128), F32), ((ROWS, 128), F32),
        ((ROWS, 256), BF16), ((ROWS, 128), F32), ((ROWS, 128), F32), ((128, 128), F32), ((128, 128), F32),
        ((ROWS, 128), F32), ((8, 16, 128), F32), ((32, 128), BF16), ((32, 128), BF16), ((NY, 128, 128), BF16),
        ((4, 64, 128), F32), ((NZ, 32, 128), BF16), ((NY, 16, 128), BF16), ((ROWS, 128), BF16), ((ROWS, 256), BF16),
        ((4, 128, D), BF16), ((4, 128, D), BF16), ((128, D), BF16), ((128, D), BF16), ((128, D), BF16),
        ((128, 1024), BF16), ((128, 1024), BF16), ((128, D), BF16), ((128, D), BF16), ((128, D), F32),
    ]
    counts = [(1,), (7,), (3,), (15,), (3,), (4, 2), (6,), (6,), (8,), (3, 16), (3, 16, 4)]
    scratch = [pltpu.VMEM(s, t) for s, t in shapes] + [dma] + [dma(n) for n in counts for _ in (0, 1)]
    return pl.pallas_call(
        layer,
        out_shape=jax.ShapeDtypeStruct((128, D), BF16),
        in_specs=[pl.BlockSpec(memory_space=pl.ANY)] + [vm] * 16,
        out_specs=vm,
        scratch_shapes=scratch,
        compiler_params=pltpu.CompilerParams(
            collective_id=0, has_side_effects=True, vmem_limit_bytes=60 * 1024 * 1024
        ),
    )(
        tokens, norm_gain.reshape(16, 128), w_conv_a, w_conv_gate, conv_weight, conv_gain.reshape(1, 128),
        w_query, w_key, w_value, w_outgate, w_decay, decay_bias.reshape(1, 64), decay_extra.T,
        head_gain.reshape(1, 128), init_state.reshape(64, 128), w_out_conv.T, w_out_gla.T,
    )


def solution(mesh):
    torus = Mesh(mesh.devices.reshape(NZ, NY, NX, NC), ("z", "y", "x", "c"))
    placed = (
        P(SP, TP),
        P(),
        P(SP, TP),
        P(SP, TP),
        P(None, TP),
        P(TP),
        P(SP, TP),
        P(SP, TP),
        P(SP, TP),
        P(SP, TP),
        P(SP, TP),
        P(TP),
        P(SP, TP),
        P(),
        P(TP, None, None),
        P(TP, SP),
        P(TP, SP),
    )
    return jax.shard_map(
        per_device, mesh=torus, in_specs=placed, out_specs=P(SP_TP, None), check_vma=False
    )
```

```python
import jax
import jax.numpy as jnp
from jax import lax
from jax.experimental import pallas as pl
from jax.experimental.pallas import tpu as pltpu
from jax.sharding import Mesh
from jax.sharding import PartitionSpec as P

D = 2048
D_CONV = 1024
ROWS = 1024
TAPS = 31
NZ, NY, NX, NC = 16, 4, 4, 2
SP = ("z", "y")
TP = ("x", "c")
SP_TP = ("z", "y", "x", "c")
PARTS = ((0, 80), (80, 144), (144, 176), (176, 240))
PAIRS = ((0,), (1, 2), (3, 4), (5, 6), (7, 8))
F32, BF16 = jnp.float32, jnp.bfloat16

epsilon = 1e-06
gate_divisor = 16.0


def remote(src, dst, send, recv, **ids):
    return pltpu.make_async_remote_copy(
        src_ref=src,
        dst_ref=dst,
        send_sem=send,
        recv_sem=recv,
        device_id=ids,
        device_id_type=pl.DeviceIdType.MESH,
    )


def send(ref, sent, recv, **ids):
    remote(ref, ref, sent, recv, **ids).start()


def arrived(ref, recv, **ids):
    remote(ref, ref, recv, recv, **ids).wait_recv()


def left(ref, sent, **ids):
    remote(ref, ref, sent, sent, **ids).wait_send()


def pack_chunk(sp, gain, wa, wg, wq, wk, wv, wo, wd, woc, wog, G):
    row = gain[pl.ds(sp // 4, 1), :]
    r = lax.broadcasted_iota(jnp.int32, (32, 128), 0)
    lane = lax.broadcasted_iota(jnp.int32, (32, 128), 1)
    mine = lane == r + 32 * lax.rem(sp, 4)
    col = jnp.sum(jnp.where(mine, jnp.broadcast_to(row, (32, 128)), 0.0), axis=1, keepdims=True)

    def scaled(ref):
        return ref[...].astype(F32) * col

    d = scaled(wd)
    G[sp, 0:32] = scaled(wv).astype(BF16)
    G[sp, 32:64] = jnp.concatenate([scaled(wq), scaled(wk)], axis=1).astype(BF16)
    G[sp, 64:80] = jnp.concatenate([d[0:16], d[16:32]], axis=1).astype(BF16)
    G[sp, 80:112] = scaled(wa).astype(BF16)
    G[sp, 112:144] = scaled(wg).astype(BF16)
    G[sp, 144:176] = scaled(wo).astype(BF16)
    G[sp, 176:208] = woc[...]
    G[sp, 208:240] = wog[...]


def greet(z, y, x, c):
    barrier = pltpu.get_barrier_semaphore()
    partners = [dict(z=lax.rem(z + d, NZ)) for d in (1, 2, NZ - 2, NZ - 1)]
    partners += [dict(y=lax.rem(y + d, NY)) for d in (1, NY - 1)]
    partners += [dict(x=lax.rem(x + d, NX)) for d in (1, NX - 1)]
    partners += [dict(c=1 - c)]
    for ids in partners:
        pl.semaphore_signal(barrier, inc=1, device_id=ids, device_id_type=pl.DeviceIdType.MESH)
    pl.semaphore_wait(barrier, len(partners))


def peer(x, c, r):
    return dict(x=lax.rem(x + r // 2, NX), c=1 - c if r % 2 else c)


def following(z, y, d):
    sp = lax.rem(z * NY + y + d + NZ * NY, NZ * NY)
    return dict(z=sp // NY, y=lax.rem(sp, NY))


class Weights:
    def __init__(self, z, y, G, zs, zr, ys, yr, fs, fr):
        self.z, self.y, self.G = z, y, G
        self.zs, self.zr, self.ys, self.yr, self.fs, self.fr = zs, zr, ys, yr, fs, fr
        self.up, self.down, self.over = (lax.rem(y + d, NY) for d in (1, 3, 2))

    def chunk(self, o, y, first, last):
        return self.G.at[lax.rem(self.z - o + NZ, NZ) * NY + y, first:last]

    def several(self, p, n):
        return self.G.at[0:n, PARTS[p][0] : PARTS[p][1]]

    def cuts(self, p, o):
        first, last = PARTS[p]
        return first, first + (48, 32)[o % 2] if p == 0 else (first + last) // 2, last

    def signs(self, a):
        return (a,) if a in (0, 8) else (a, -a)

    def z_out(self, p, o):
        step = (2 if abs(o) > 1 else 1) * (1 if o > 0 else -1)
        send(self.chunk(o - step, self.y, *PARTS[p]), self.zs.at[p], self.zr.at[p, o + 7], z=lax.rem(self.z + step + NZ, NZ))

    def y_out(self, p, o):
        for k, to in enumerate((self.up, self.down)):
            send(self.chunk(o, self.y, *PARTS[p]), self.ys.at[p], self.yr.at[p, abs(o), k], y=to)

    def begin_z(self, p):
        for o in (1, -1, 2, -2):
            self.z_out(p, o)

    def begin(self, p):
        self.begin_z(p)
        self.y_out(p, 0)

    def cross(self, p, pair):
        for a in pair:
            for o in self.signs(a):
                self.y_out(p, o)

    def relay(self, p, pair, cross=True):
        for a in pair:
            for o in self.signs(a):
                arrived(self.chunk(o, self.y, *PARTS[p]), self.zr.at[p, o + 7], z=lax.rem(self.z + 1, NZ))
                further = o + 2 if o > 0 else o - 2
                if -7 <= further <= 8:
                    self.z_out(p, further)
                if cross:
                    self.y_out(p, o)

    def forward(self, p, pair):
        for a in pair:
            both = self.several(p, len(self.signs(a)))
            arrived(both, self.yr.at[p, a, 0], y=self.down)
            for o in self.signs(a):
                first, middle, last = self.cuts(p, o)
                send(self.chunk(o, self.down, first, middle), self.fs.at[p], self.fr.at[p], y=self.up)
            arrived(both, self.yr.at[p, a, 1], y=self.up)
            for o in self.signs(a):
                first, middle, last = self.cuts(p, o)
                send(self.chunk(o, self.up, middle, last), self.fs.at[p], self.fr.at[p], y=self.down)

    def end(self, p):
        arrived(self.several(p, 16), self.fr.at[p], y=self.down)

    def drain(self, p):
        left(self.several(p, 15), self.zs.at[p], y=self.down)
        left(self.several(p, 32), self.ys.at[p], y=self.down)
        left(self.several(p, 16), self.fs.at[p], y=self.down)


class Tokens:
    def __init__(self, x, c, tok, ssq, xs, xr, ds, dr):
        self.c, self.tok, self.ssq = c, tok, ssq
        self.xs, self.xr, self.ds, self.dr = xs, xr, ds, dr
        self.x, self.right, self.left, self.over = (lax.rem(x + d, NX) for d in (0, 1, 3, 2))
        self.order = [
            (self.x, 0), (self.x, 1), (self.left, 0), (self.right, 1),
            (self.left, 1), (self.right, 0), (self.over, 0), (self.over, 1),
        ]

    def slab(self, xi, ci, half):
        col = pl.multiple_of((xi * NC + ci) * 256, 256)
        return self.tok.at[pl.ds(half * 512, 512), pl.ds(col, 256)]

    def send(self, xi, half, k, to):
        send(self.slab(xi, self.c, half), self.xs.at[0], self.xr.at[k], x=to)

    def begin(self):
        self.send(self.x, 0, 0, self.right)
        self.send(self.x, 1, 1, self.left)
        self.send(self.x, 1, 2, self.right)
        self.send(self.x, 0, 3, self.left)
        self.across(0)
        self.across(1)

    def across(self, k):
        send(self.slab(self.order[k][0], self.c, self.order[k][1]), self.ds.at[0], self.dr.at[k], c=1 - self.c)

    def drain(self):
        left(self.tok.at[:, 0:768], self.xs.at[0], c=1 - self.c)
        left(self.tok.at[:, 0:1024], self.ds.at[0], c=1 - self.c)

    def take(self, k):
        xi, half = self.order[k]
        arrived(self.slab(xi, self.c, half), self.xr.at[k - 2], x=self.right if k % 2 else self.left)
        if k == 2:
            self.send(xi, half, 4, self.right)
        if k == 3:
            self.send(xi, half, 5, self.left)
        self.across(k)

    def take_across(self, k):
        xi, half = self.order[k]
        arrived(self.slab(xi, 1 - self.c, half), self.dr.at[k], c=1 - self.c)

    def squares(self, k, ci):
        xi, half = self.order[k]
        rows = slice(half * 512, half * 512 + 512)
        t = self.slab(xi, ci, half)[...].astype(F32)
        self.ssq[rows, :] += t[:, 0:128] * t[:, 0:128] + t[:, 128:256] * t[:, 128:256]


def unpack_decay(G, Wd):
    def step(k, _):
        rows = pl.ds(pl.multiple_of(k * 256, 256), 256)
        d = G[pl.ds(k * 8, 8), 64:80, :].astype(F32)
        both = jnp.concatenate([d[:, :, 0:64], d[:, :, 64:128]], axis=1).reshape(256, 64)
        Wd[rows, :] = jnp.concatenate([both, both], axis=1).astype(BF16)
        return 0

    lax.fori_loop(0, 8, step, 0)


def column(G, first):
    return G[:, first : first + 32, :].reshape(D, 128)


def nt(a, b):
    return lax.dot_general(a, b, (((1,), (1,)), ((), ())), preferred_element_type=F32)


def tn(a, b):
    return lax.dot_general(a, b, (((0,), (0,)), ((), ())), preferred_element_type=F32)


def nn(a, b):
    return jnp.dot(a, b, preferred_element_type=F32)


def again(x):
    return x.astype(BF16).astype(F32)


def iota(shape, axis):
    return lax.broadcasted_iota(jnp.int32, shape, axis)


def project_first(i, tok, G, Wd, ssq, v, qk, dec):
    rows = slice(256 * i, 256 * i + 256)
    t = tok[rows, :]
    scale = lax.rsqrt(jnp.sum(ssq[rows, :], axis=1, keepdims=True) * (1.0 / D) + epsilon)
    ssq[rows, :] = jnp.broadcast_to(scale, (256, 128))
    part = nn(t, jnp.concatenate([column(G, 0), column(G, 32)], axis=1)) * scale
    v[rows, :] = part[:, 0:128].astype(BF16)
    qk[rows, :] = again(part[:, 128:256])
    dec[rows, :] = nn(t, Wd[...]) * scale


def project_second(i, tok, G, ssq, gext):
    rows = slice(256 * i, 256 * i + 256)
    t = tok[rows, :]
    scale = ssq[rows, :]
    part = nn(t, jnp.concatenate([column(G, 80), column(G, 112)], axis=1))
    gated = again(part[:, 0:128] * scale) * jax.nn.sigmoid(again(part[:, 128:256] * scale))
    gext[256 * i + 32 : 256 * i + 288, :] = again(gated)


def project_third(i, tok, G, ssq, og):
    rows = slice(256 * i, 256 * i + 256)
    og[rows, :] = (nn(tok[rows, :], column(G, 144)) * ssq[rows, :]).astype(BF16)


def split_heads(qk, rows):
    low = iota((256, 128), 1) < 64
    a = qk[rows, :]
    b = pltpu.roll(a, 64, 1)
    return low, jnp.where(low, a, b) * 0.125, jnp.where(low, b, a)


def same_block():
    r, s = iota((256, 256), 0), iota((256, 256), 1)
    return r // 64 == s // 64, s <= r


def block_states(i, bias, extra, dec, qk, v, kv, tots):
    rows = slice(i * 256, i * 256 + 256)
    pre = dec[rows, :] + bias
    log = jnp.minimum(pre, 0.0) - jnp.log1p(jnp.exp(-jnp.abs(pre)))
    cum = log * (1.0 / gate_divisor) + extra[rows, :]
    place = lax.rem(iota((256, 128), 0), 64)
    for s in (1, 2, 4, 8, 16, 32):
        cum = cum + jnp.where(place >= s, pltpu.roll(cum, s, 0), 0.0)
    dec[rows, :] = cum
    total = cum.reshape(4, 64, 128)[:, 63:64, :]
    tots[4 * i : 4 * i + 4, :] = total.reshape(4, 128)
    total = jnp.broadcast_to(total, (4, 64, 128)).reshape(256, 128)
    _, _, k = split_heads(qk, rows)
    to_end = k * jnp.exp(total - cum)
    same, _ = same_block()
    spread = jnp.where(same, jnp.concatenate([to_end, to_end], axis=1), 0.0).astype(BF16)
    kv[rows, :] = tn(spread, v[rows, :])


def block_scores(i, dec, qk, v, Q, within):
    rows = slice(i * 256, i * 256 + 256)
    cum = dec[rows, :]
    low, q, k = split_heads(qk, rows)
    q = q * jnp.exp(cum)
    inverse = k * jnp.exp(-cum)
    same, causal = same_block()
    scores = nt(jnp.where(low, q, 0.0).astype(BF16), inverse.astype(BF16))
    scores = jnp.where(same & causal, scores, 0.0).astype(BF16)
    Q[rows, :] = jnp.where(same, jnp.concatenate([q, q], axis=1), 0.0).astype(BF16)
    within[rows, :] = nn(scores, v[rows, :])


def conv_sums(cw, gext, csum, mine):
    for b in range(8):
        acc = jnp.zeros((128, 128), F32)
        for j in range(TAPS):
            acc = acc + cw[j : j + 1, :] * gext[128 * b + 2 + j : 128 * b + 130 + j, :]
        csum[128 * b : 128 * b + 128, :] = acc
        t = acc.T
        mine[b : b + 1, :] = jnp.sum(t, axis=0, keepdims=True)
        mine[8 + b : 9 + b, :] = jnp.sum(t * t, axis=0, keepdims=True)


def conv_finish(cst, square, csum, conv_gain, X):
    both = cst[0]
    for k in range(1, 8):
        both = both + cst[k]
    both = both * (1.0 / D_CONV)
    mean = both[0:8]
    square[0:8, :] = mean
    square[8:16, :] = lax.rsqrt(both[8:16] - mean * mean + epsilon)
    t = square[...].T
    for b in range(8):
        n = (csum[128 * b : 128 * b + 128, :] - t[:, b : b + 1]) * t[:, 8 + b : 9 + b] * conv_gain
        X[128 * b : 128 * b + 128, 0:128] = (n * jax.nn.sigmoid(n)).astype(BF16)


def layer(tokens, gain, wa, wg, cw, conv_gain, wq, wk, wv, wo, wd, bias, extra_t, head_gain, init, woc, wog,
          out, G, tok, Wd, ssq, gext, v, og, qk, dec, extra, Q, within, kv, tots, square, csum, cst, hout, hin, ybuf,
          ztot, zbuf, fbuf, Sst, X, pout, pin, s0, s1, s2, r0, r1, fl, fr, facc,
          local, hs, hr, cs, cr, ys, yr, zs, zr, fs, fr_, ps, pr, gs, gr, xs, xr_, ds, dr, wzs, wzr, wys, wyr, wfs, wfr):
    z, y, x, c = (lax.axis_index(n) for n in ("z", "y", "x", "c"))
    sp = z * NY + y
    tp = x * NC + c
    t = Tokens(x, c, tok, ssq, xs, xr_, ds, dr)
    w = Weights(z, y, G, wzs, wzr, wys, wyr, wfs, wfr)
    own = pltpu.make_async_copy(tokens, tok.at[:, pl.ds(pl.multiple_of(tp * 256, 256), 256)], local)
    own.start()
    pack_chunk(sp, gain, wa, wg, wq, wk, wv, wo, wd, woc, wog, G)
    zbuf[...] = jnp.zeros_like(zbuf)
    greet(z, y, x, c)

    w.begin(0)
    own.wait()
    t.begin()
    w.begin(1)
    for b in range(8):
        e = extra_t[:, 128 * b : 128 * b + 128]
        extra[128 * b : 128 * b + 128, :] = jnp.concatenate([e, e], axis=0).T
    tots[...] = jnp.zeros_like(tots)
    square[...] = jnp.zeros_like(square)
    ssq[...] = jnp.zeros_like(ssq)
    t.squares(0, c)
    t.squares(1, c)
    w.relay(0, PAIRS[1])
    w.forward(0, PAIRS[0])
    w.relay(1, PAIRS[1])
    w.relay(0, PAIRS[2])
    w.forward(0, PAIRS[1])
    t.take(2)
    t.take(3)
    w.relay(1, PAIRS[2])
    w.forward(1, PAIRS[0])
    w.begin_z(2)
    for k in (0, 1):
        t.take_across(k)
        t.squares(k, 1 - c)
    w.relay(0, PAIRS[3])
    w.forward(0, PAIRS[2])
    w.relay(1, PAIRS[3], False)
    w.forward(1, PAIRS[1])
    w.begin_z(3)
    w.relay(2, PAIRS[1], False)
    w.relay(0, PAIRS[4])
    w.forward(0, PAIRS[3])
    t.take(4)
    t.take(5)
    w.relay(1, PAIRS[4], False)
    for k in (2, 3):
        t.squares(k, c)
        t.take_across(k)
        t.squares(k, 1 - c)
    w.relay(3, PAIRS[1], False)
    w.relay(2, PAIRS[2], False)
    w.forward(0, PAIRS[4])
    w.cross(1, PAIRS[3])
    w.cross(1, PAIRS[4])
    w.forward(1, PAIRS[2])
    for k in (4, 5):
        t.squares(k, c)
        t.take_across(k)
        t.squares(k, 1 - c)
    t.take(6)
    t.take(7)
    w.relay(3, PAIRS[2], False)
    w.relay(2, PAIRS[3], False)
    w.end(0)
    unpack_decay(G, Wd)
    for k in (6, 7):
        t.squares(k, c)
        t.take_across(k)
        t.squares(k, 1 - c)

    for i in range(4):
        project_first(i, tok, G, Wd, ssq, v, qk, dec)
        if i == 1:
            w.forward(1, PAIRS[3])
    w.relay(3, PAIRS[3], False)
    w.relay(2, PAIRS[4], False)
    b2 = jnp.concatenate([bias[...], bias[...]], axis=1)
    for i in range(4):
        block_states(i, b2, extra, dec, qk, v, kv, tots)
        if i == 1:
            w.forward(1, PAIRS[4])
    tt = tots[...].T[0:64, :]
    decay = jnp.exp(tt)
    state = jnp.zeros((64, 128), F32)
    for b in range(16):
        state = state * decay[:, b : b + 1] + kv[64 * b : 64 * b + 64, :]
    ybuf[y, 0:64] = state.astype(BF16)
    ybuf[y, 64:128] = jnp.broadcast_to(jnp.exp(jnp.sum(tt, axis=1, keepdims=True)), (64, 128)).astype(BF16)
    for d in (2, 1, 3):
        send(ybuf.at[y], ys.at[0], yr.at[0], y=lax.rem(y + d, NY))
    for pair in PAIRS:
        w.cross(2, pair)
    for pair in PAIRS[0:4]:
        w.cross(3, pair)
    for i in range(4):
        block_scores(i, dec, qk, v, Q, within)
    w.relay(3, PAIRS[4])

    arrived(ybuf.at[0:3], yr.at[0], y=lax.rem(y + 1, NY))
    row_state = jnp.zeros((64, 128), F32)
    row_decay = jnp.ones((64, 128), F32)
    pre_state, pre_decay = row_state, row_decay
    for k in range(NY):
        pre_state = jnp.where(y == k, row_state, pre_state)
        pre_decay = jnp.where(y == k, row_decay, pre_decay)
        a = ybuf[k, 64:128].astype(F32)
        row_state = row_state * a + ybuf[k, 0:64].astype(F32)
        row_decay = row_decay * a
    ztot[0] = row_state
    ztot[1] = row_decay
    ztot[2] = pre_state
    ztot[3] = pre_decay
    part = pl.ds(pl.multiple_of(y * 16, 16), 16)
    zbuf[z, 0:16] = ztot[0, part, :].astype(BF16)
    low = iota((8, 128), 1) < 64
    a = ztot[1, part, :]
    zbuf[z, 16:24] = jnp.where(low, a[0:8], a[8:16]).astype(BF16)
    for d in range(NZ - 1, 0, -1):
        @pl.when(z + d < NZ)
        def _():
            remote(zbuf.at[z], zbuf.at[z], zs.at[d - 1], zr.at[d - 1], z=lax.rem(z + d, NZ)).start()

    w.end(1)

    for i in range(4):
        project_second(i, tok, G, ssq, gext)
    hout[...] = gext[ROWS : ROWS + 32, :].astype(BF16)
    after, ahead = following(z, y, 1), following(z, y, -1)
    halo = remote(hout, hin, hs.at[0], hr.at[0], **after)
    halo.start()

    for pair in PAIRS:
        w.forward(2, pair)
    halo.wait_send()
    remote(hout, hin, hs.at[0], hr.at[0], **ahead).wait_recv()
    gext[0:32, :] = jnp.where(sp > 0, hin[...].astype(F32), 0.0)
    conv_sums(cw, gext, csum, cst.at[tp])
    for r in range(1, 8):
        send(cst.at[tp], cs.at[0], cr.at[0], **peer(x, c, r))
    for pair in PAIRS[0:3]:
        w.forward(3, pair)
    w.end(2)
    for i in range(4):
        project_third(i, tok, G, ssq, og)
    for pair in PAIRS[3:5]:
        w.forward(3, pair)

    arrived(cst.at[0:7], cr.at[0], c=1 - c)
    conv_finish(cst, square, csum, conv_gain[...], X)

    for d in range(1, NZ):
        @pl.when(z >= d)
        def _():
            zd = lax.rem(z + NZ - d, NZ)
            arrived(zbuf.at[zd], zr.at[d - 1], z=zd)
    state = init[part, :]
    for k in range(NZ - 1):
        a = zbuf[k, 16:24].astype(F32)
        b = pltpu.roll(a, 64, 1)
        a = jnp.concatenate([jnp.where(low, a, b), jnp.where(low, b, a)], axis=0)
        following_state = state * a + zbuf[k, 0:16].astype(F32)
        state = jnp.where(k < z, following_state, state)
    fbuf[y] = state.astype(BF16)
    for d in (2, 1, 3):
        send(fbuf.at[y], fs.at[0], fr_.at[0], y=lax.rem(y + d, NY))
    arrived(fbuf.at[0:3], fr_.at[0], y=lax.rem(y + 1, NY))
    state = fbuf[...].reshape(64, 128).astype(F32) * ztot[3] + ztot[2]
    for b in range(16):
        Sst[64 * b : 64 * b + 64, :] = state.astype(BF16)
        state = state * decay[:, b : b + 1] + kv[64 * b : 64 * b + 64, :]

    def finish(xi):
        rows = pl.ds(pl.multiple_of(xi * 256, 256), 256)
        attn = within[rows, :] + nn(Q[rows, :], Sst[rows, :])
        mean = jnp.sum(attn * attn, axis=1, keepdims=True) * (1.0 / 128.0)
        o = og[rows, :].astype(F32)
        X[rows, 128:256] = (
            attn * lax.rsqrt(mean + epsilon) * head_gain[...] * (o * jax.nn.sigmoid(o))
        ).astype(BF16)

    right, back, over = lax.rem(x + 1, NX), lax.rem(x + NX - 1, NX), lax.rem(x + 2, NX)
    order = (over, right, back, x)

    def product(xi, ci, n):
        rows = pl.ds(pl.multiple_of((xi * NC + ci) * 128, 128), 128)
        cols = slice(16 * n, 16 * n + 16)
        wt = jnp.concatenate([G[cols, 176:208, :].reshape(512, 128), G[cols, 208:240, :].reshape(512, 128)], axis=1)
        return nt(X[rows, :], wt)

    def half(h):
        return slice(1024 * h, 1024 * h + 1024)

    def pair(q, h):
        return remote(pout.at[q, :, half(h)], pin.at[q, :, half(h)], ps.at[0], pr.at[q, h], c=1 - c)

    def for_pair(q, h):
        for n in (2 * h, 2 * h + 1):
            pout[q, :, 512 * n : 512 * n + 512] = product(order[q], 1 - c, n).astype(BF16)
        pair(q, h).start()

    def pair_sum(q, h, to):
        mine = [product(order[q], c, n) for n in (2 * h, 2 * h + 1)]
        pair(q, h).wait_recv()
        for n, value in zip((2 * h, 2 * h + 1), mine):
            cols = slice(512 * n, 512 * n + 512)
            to[:, cols] = (value + pin[q, :, cols].astype(F32)).astype(to.dtype)

    def ring(k, src, dst, xi):
        remote(src, dst, gs.at[0], gr.at[k], x=xi).start()

    def ring_in(k, dst, xi):
        arrived(dst, gr.at[k], x=xi)

    finish(over)
    w.end(3)
    for_pair(0, 0)
    for_pair(0, 1)
    finish(right)
    pair_sum(0, 0, s0)
    ring(0, s0.at[:, half(0)], r0, right)
    for_pair(1, 1)
    pair_sum(0, 1, s0)
    ring(1, s0.at[:, half(1)], r1, back)
    finish(back)
    for_pair(2, 0)
    pair_sum(1, 1, s1)
    ring(2, s1.at[:, half(1)], fl.at[:, half(1)], right)
    for_pair(1, 0)
    pair_sum(2, 0, s2)
    ring(3, s2.at[:, half(0)], fr.at[:, half(0)], back)
    for_pair(2, 1)
    finish(x)
    pair_sum(1, 0, s1)
    for_pair(3, 0)
    pair_sum(2, 1, s2)
    for_pair(3, 1)
    ring_in(0, r0, back)
    s1[:, half(0)] = (s1[:, half(0)].astype(F32) + r0[...].astype(F32)).astype(BF16)
    ring(4, s1.at[:, half(0)], fl.at[:, half(0)], right)
    ring_in(1, r1, right)
    s2[:, half(1)] = (s2[:, half(1)].astype(F32) + r1[...].astype(F32)).astype(BF16)
    ring(5, s2.at[:, half(1)], fr.at[:, half(1)], back)
    pair_sum(3, 0, facc)
    pair_sum(3, 1, facc)
    for p in range(4):
        w.drain(p)
    t.drain()
    left(ybuf.at[0:3], ys.at[0], y=after["y"])
    left(fbuf.at[0:3], fs.at[0], y=after["y"])
    left(cst.at[0:7], cs.at[0], c=1 - c)
    left(pout, ps.at[0], c=1 - c)
    for d in range(1, NZ):
        @pl.when(z + d < NZ)
        def _():
            left(zbuf.at[z], zs.at[d - 1], z=lax.rem(z + d, NZ))
    ring_in(2, fl.at[:, half(1)], back)
    ring_in(3, fr.at[:, half(0)], right)
    facc[:, half(0)] += fr[:, half(0)].astype(F32)
    facc[:, half(1)] += fl[:, half(1)].astype(F32)
    ring_in(4, fl.at[:, half(0)], back)
    out[:, half(0)] = (facc[:, half(0)] + fl[:, half(0)].astype(F32)).astype(BF16)
    ring_in(5, fr.at[:, half(1)], right)
    out[:, half(1)] = (facc[:, half(1)] + fr[:, half(1)].astype(F32)).astype(BF16)
    left(pout.at[0:3], gs.at[0], x=right)


def per_device(
    tokens, norm_gain, w_conv_a, w_conv_gate, conv_weight, conv_gain, w_query, w_key, w_value,
    w_outgate, w_decay, decay_bias, decay_extra, head_gain, init_state, w_out_conv, w_out_gla,
):
    vm = pl.BlockSpec(memory_space=pltpu.VMEM)
    dma = pltpu.SemaphoreType.DMA
    shapes = [
        ((64, 240, 128), BF16), ((ROWS, D), BF16), ((D, 128), BF16), ((ROWS, 128), F32), ((ROWS + 32, 128), F32),
        ((ROWS, 128), BF16), ((ROWS, 128), BF16), ((ROWS, 128), F32), ((ROWS, 128), F32), ((ROWS, 128), F32),
        ((ROWS, 256), BF16), ((ROWS, 128), F32), ((ROWS, 128), F32), ((128, 128), F32), ((128, 128), F32),
        ((ROWS, 128), F32), ((8, 16, 128), F32), ((32, 128), BF16), ((32, 128), BF16), ((NY, 128, 128), BF16),
        ((4, 64, 128), F32), ((NZ, 24, 128), BF16), ((NY, 16, 128), BF16), ((ROWS, 128), BF16), ((ROWS, 256), BF16),
        ((4, 128, D), BF16), ((4, 128, D), BF16), ((128, D), BF16), ((128, D), BF16), ((128, D), BF16),
        ((128, 1024), BF16), ((128, 1024), BF16), ((128, D), BF16), ((128, D), BF16), ((128, D), F32),
    ]
    counts = [
        (1,), (1,), (1,), (1,), (1,), (1,), (15,), (15,), (1,), (1,), (1,), (4, 2), (1,), (6,),
        (1,), (6,), (1,), (8,), (4,), (4, 16), (4,), (4, 9, 2), (4,), (4,),
    ]
    scratch = [pltpu.VMEM(s, t) for s, t in shapes] + [dma] + [dma(n) for n in counts]
    return pl.pallas_call(
        layer,
        out_shape=jax.ShapeDtypeStruct((128, D), BF16),
        in_specs=[pl.BlockSpec(memory_space=pl.ANY)] + [vm] * 16,
        out_specs=vm,
        scratch_shapes=scratch,
        compiler_params=pltpu.CompilerParams(
            collective_id=0, has_side_effects=True, vmem_limit_bytes=60 * 1024 * 1024
        ),
    )(
        tokens, norm_gain.reshape(16, 128), w_conv_a, w_conv_gate, conv_weight, conv_gain.reshape(1, 128),
        w_query, w_key, w_value, w_outgate, w_decay, decay_bias.reshape(1, 64), decay_extra.T,
        head_gain.reshape(1, 128), init_state.reshape(64, 128), w_out_conv.T, w_out_gla.T,
    )


def solution(mesh):
    torus = Mesh(mesh.devices.reshape(NZ, NY, NX, NC), ("z", "y", "x", "c"))
    placed = (
        P(SP, TP),
        P(),
        P(SP, TP),
        P(SP, TP),
        P(None, TP),
        P(TP),
        P(SP, TP),
        P(SP, TP),
        P(SP, TP),
        P(SP, TP),
        P(SP, TP),
        P(TP),
        P(SP, TP),
        P(),
        P(TP, None, None),
        P(TP, SP),
        P(TP, SP),
    )
    return jax.shard_map(
        per_device, mesh=torus, in_specs=placed, out_specs=P(SP_TP, None), check_vma=False
    )
```

```python
import jax
import jax.numpy as jnp
from jax import lax
from jax.experimental import pallas as pl
from jax.experimental.pallas import tpu as pltpu
from jax.sharding import Mesh
from jax.sharding import PartitionSpec as P

D = 2048
D_CONV = 1024
ROWS = 1024
TAPS = 31
NZ, NY, NX, NC = 16, 4, 4, 2
SP = ("z", "y")
TP = ("x", "c")
SP_TP = ("z", "y", "x", "c")
PARTS = ((0, 80), (80, 144), (144, 176), (208, 240), (176, 208))
PAIRS = ((0,), (1, 2), (3, 4), (5, 6), (7, 8))
EARLY, LATE = (0, 1, 2, 5, 6, 7, 8, 9, 14, 15), (3, 4, 10, 11, 12, 13)
F32, BF16 = jnp.float32, jnp.bfloat16

epsilon = 1e-06
gate_divisor = 16.0


def remote(src, dst, send, recv, **ids):
    return pltpu.make_async_remote_copy(
        src_ref=src,
        dst_ref=dst,
        send_sem=send,
        recv_sem=recv,
        device_id=ids,
        device_id_type=pl.DeviceIdType.MESH,
    )


def send(ref, sent, recv, **ids):
    remote(ref, ref, sent, recv, **ids).start()


def arrived(ref, recv, **ids):
    remote(ref, ref, recv, recv, **ids).wait_recv()


def left(ref, sent, **ids):
    remote(ref, ref, sent, sent, **ids).wait_send()


def pack_chunk(sp, gain, wa, wg, wq, wk, wv, wo, wd, woc, wog, G):
    row = gain[pl.ds(sp // 4, 1), :]
    r = lax.broadcasted_iota(jnp.int32, (32, 128), 0)
    lane = lax.broadcasted_iota(jnp.int32, (32, 128), 1)
    mine = lane == r + 32 * lax.rem(sp, 4)
    col = jnp.sum(jnp.where(mine, jnp.broadcast_to(row, (32, 128)), 0.0), axis=1, keepdims=True)

    def scaled(ref):
        return ref[...].astype(F32) * col

    d = scaled(wd)
    G[sp, 0:32] = scaled(wv).astype(BF16)
    G[sp, 32:64] = jnp.concatenate([scaled(wq), scaled(wk)], axis=1).astype(BF16)
    G[sp, 64:80] = jnp.concatenate([d[0:16], d[16:32]], axis=1).astype(BF16)
    G[sp, 80:112] = scaled(wa).astype(BF16)
    G[sp, 112:144] = scaled(wg).astype(BF16)
    G[sp, 144:176] = scaled(wo).astype(BF16)
    G[sp, 176:208] = woc[...]
    G[sp, 208:240] = wog[...]


def greet_all():
    z, y, x, c = (lax.axis_index(n) for n in ("z", "y", "x", "c"))
    barrier = pltpu.get_barrier_semaphore()
    partners = [dict(z=lax.rem(z + d, NZ)) for d in (1, 2, NZ - 2, NZ - 1)]
    partners += [dict(y=lax.rem(y + d, NY)) for d in (1, NY - 1)]
    partners += [dict(x=lax.rem(x + d, NX)) for d in (1, NX - 1)]
    partners += [dict(c=1 - c)]
    for ids in partners:
        pl.semaphore_signal(barrier, inc=1, device_id=ids, device_id_type=pl.DeviceIdType.MESH)


def greet_wait():
    pl.semaphore_wait(pltpu.get_barrier_semaphore(), 9)


def peer(x, c, r):
    return dict(x=lax.rem(x + r // 2, NX), c=1 - c if r % 2 else c)


def following(z, y, d):
    sp = lax.rem(z * NY + y + d + NZ * NY, NZ * NY)
    return dict(z=sp // NY, y=lax.rem(sp, NY))


class Weights:
    def __init__(self, z, y, G, zs, zr, ys, yr, fs, fr):
        self.z, self.y, self.G = z, y, G
        self.zs, self.zr, self.ys, self.yr, self.fs, self.fr = zs, zr, ys, yr, fs, fr
        self.up, self.down, self.over = (lax.rem(y + d, NY) for d in (1, 3, 2))

    def chunk(self, o, y, first, last):
        return self.G.at[lax.rem(self.z - o + NZ, NZ) * NY + y, first:last]

    def several(self, p, n):
        return self.G.at[0:n, PARTS[p][0] : PARTS[p][1]]

    def cuts(self, p, o):
        first, last = PARTS[p]
        return first, first + (48, 32)[o % 2] if p == 0 else (first + last) // 2, last

    def signs(self, a):
        return (a,) if a in (0, 8) else (a, -a)

    def z_out(self, p, o):
        step = (2 if abs(o) > 1 else 1) * (1 if o > 0 else -1)
        send(self.chunk(o - step, self.y, *PARTS[p]), self.zs.at[p], self.zr.at[p, o + 7], z=lax.rem(self.z + step + NZ, NZ))

    def y_out(self, p, o):
        for k, to in enumerate((self.up, self.down)):
            send(self.chunk(o, self.y, *PARTS[p]), self.ys.at[p], self.yr.at[p, abs(o), k], y=to)

    def begin_z(self, p):
        for o in (1, -1, 2, -2):
            self.z_out(p, o)

    def begin(self, p):
        self.begin_z(p)
        self.y_out(p, 0)

    def cross(self, p, pair):
        for a in pair:
            for o in self.signs(a):
                self.y_out(p, o)

    def relay(self, p, pair, cross=True):
        for a in pair:
            for o in self.signs(a):
                arrived(self.chunk(o, self.y, *PARTS[p]), self.zr.at[p, o + 7], z=lax.rem(self.z + 1, NZ))
                further = o + 2 if o > 0 else o - 2
                if -7 <= further <= 8:
                    self.z_out(p, further)
                if cross:
                    self.y_out(p, o)

    def forward(self, p, pair):
        for a in pair:
            both = self.several(p, len(self.signs(a)))
            arrived(both, self.yr.at[p, a, 0], y=self.down)
            for o in self.signs(a):
                first, middle, last = self.cuts(p, o)
                send(self.chunk(o, self.down, first, middle), self.fs.at[p], self.fr.at[p], y=self.up)
            arrived(both, self.yr.at[p, a, 1], y=self.up)
            for o in self.signs(a):
                first, middle, last = self.cuts(p, o)
                send(self.chunk(o, self.up, middle, last), self.fs.at[p], self.fr.at[p], y=self.down)

    def end(self, p):
        arrived(self.several(p, 16), self.fr.at[p], y=self.down)

    def row(self, o):
        return self.G.at[pl.ds(lax.rem(self.z - o + NZ, NZ) * NY, NY), PARTS[4][0] : PARTS[4][1]]

    def row_out(self, o):
        step = (2 if abs(o) > 1 else 1) * (1 if o > 0 else -1)
        send(self.row(o - step), self.zs.at[4], self.zr.at[4, o + 7], z=lax.rem(self.z + step + NZ, NZ))

    def rows_y(self):
        for to in (self.over, self.up, self.down):
            send(self.chunk(0, self.y, *PARTS[4]), self.ys.at[4], self.yr.at[4, 0, 0], y=to)

    def rows_begin(self):
        arrived(self.several(4, 3), self.yr.at[4, 0, 0], y=self.up)
        for o in (1, -1, 2, -2):
            self.row_out(o)

    def rows_relay(self, pair):
        for a in pair:
            for o in self.signs(a):
                arrived(self.row(o), self.zr.at[4, o + 7], z=lax.rem(self.z + 1, NZ))
                further = o + 2 if o > 0 else o - 2
                if -7 <= further <= 8:
                    self.row_out(further)

    def rows_drain(self):
        left(self.several(4, 60), self.zs.at[4], y=self.down)
        left(self.several(4, 3), self.ys.at[4], y=self.down)

    def drain(self, p):
        left(self.several(p, 15), self.zs.at[p], y=self.down)
        left(self.several(p, 32), self.ys.at[p], y=self.down)
        left(self.several(p, 16), self.fs.at[p], y=self.down)


class Tokens:
    def __init__(self, x, c, tok, ssq, xs, xr, ds, dr):
        self.c, self.tok, self.ssq = c, tok, ssq
        self.xs, self.xr, self.ds, self.dr = xs, xr, ds, dr
        self.x, self.right, self.left, self.over = (lax.rem(x + d, NX) for d in (0, 1, 3, 2))
        self.order = [
            (self.x, 0), (self.x, 1), (self.left, 0), (self.right, 1),
            (self.left, 1), (self.right, 0), (self.over, 0), (self.over, 1),
        ]

    def slab(self, xi, ci, half):
        col = pl.multiple_of((xi * NC + ci) * 256, 256)
        return self.tok.at[pl.ds(half * 512, 512), pl.ds(col, 256)]

    def send(self, xi, half, k, to):
        send(self.slab(xi, self.c, half), self.xs.at[0], self.xr.at[k], x=to)

    def begin(self):
        self.send(self.x, 0, 0, self.right)
        self.send(self.x, 1, 1, self.left)
        self.send(self.x, 1, 2, self.right)
        self.send(self.x, 0, 3, self.left)
        self.across(0)
        self.across(1)

    def across(self, k):
        send(self.slab(self.order[k][0], self.c, self.order[k][1]), self.ds.at[0], self.dr.at[k], c=1 - self.c)

    def drain(self):
        left(self.tok.at[:, 0:768], self.xs.at[0], c=1 - self.c)
        left(self.tok.at[:, 0:1024], self.ds.at[0], c=1 - self.c)

    def take(self, k):
        xi, half = self.order[k]
        arrived(self.slab(xi, self.c, half), self.xr.at[k - 2], x=self.right if k % 2 else self.left)
        if k == 2:
            self.send(xi, half, 4, self.right)
        if k == 3:
            self.send(xi, half, 5, self.left)
        self.across(k)

    def take_across(self, k):
        xi, half = self.order[k]
        arrived(self.slab(xi, 1 - self.c, half), self.dr.at[k], c=1 - self.c)

    def squares(self, k, ci):
        xi, half = self.order[k]
        rows = slice(half * 512, half * 512 + 512)
        t = self.slab(xi, ci, half)[...].astype(F32)
        self.ssq[rows, :] += t[:, 0:128] * t[:, 0:128] + t[:, 128:256] * t[:, 128:256]


def unpack_decay(G, Wd):
    def step(k, _):
        rows = pl.ds(pl.multiple_of(k * 256, 256), 256)
        d = G[pl.ds(k * 8, 8), 64:80, :].astype(F32)
        both = jnp.concatenate([d[:, :, 0:64], d[:, :, 64:128]], axis=1).reshape(256, 64)
        Wd[rows, :] = jnp.concatenate([both, both], axis=1).astype(BF16)
        return 0

    lax.fori_loop(0, 8, step, 0)


def column(G, first):
    return G[:, first : first + 32, :].reshape(D, 128)


def nt(a, b):
    return lax.dot_general(a, b, (((1,), (1,)), ((), ())), preferred_element_type=F32)


def tn(a, b):
    return lax.dot_general(a, b, (((0,), (0,)), ((), ())), preferred_element_type=F32)


def nn(a, b):
    return jnp.dot(a, b, preferred_element_type=F32)


def again(x):
    return x.astype(BF16).astype(F32)


def iota(shape, axis):
    return lax.broadcasted_iota(jnp.int32, shape, axis)


def project_first(i, tok, G, Wd, ssq, v, qk, dec):
    rows = slice(256 * i, 256 * i + 256)
    t = tok[rows, :]
    scale = lax.rsqrt(jnp.sum(ssq[rows, :], axis=1, keepdims=True) * (1.0 / D) + epsilon)
    ssq[rows, :] = jnp.broadcast_to(scale, (256, 128))
    part = nn(t, jnp.concatenate([column(G, 0), column(G, 32)], axis=1)) * scale
    v[rows, :] = part[:, 0:128].astype(BF16)
    qk[rows, :] = again(part[:, 128:256])
    dec[rows, :] = nn(t, Wd[...]) * scale


def project_second(i, tok, G, ssq, gext):
    rows = slice(256 * i, 256 * i + 256)
    t = tok[rows, :]
    scale = ssq[rows, :]
    part = nn(t, jnp.concatenate([column(G, 80), column(G, 112)], axis=1))
    gated = again(part[:, 0:128] * scale) * jax.nn.sigmoid(again(part[:, 128:256] * scale))
    gext[256 * i + 32 : 256 * i + 288, :] = again(gated)


def project_third(i, tok, G, ssq, og):
    rows = slice(256 * i, 256 * i + 256)
    og[rows, :] = (nn(tok[rows, :], column(G, 144)) * ssq[rows, :]).astype(BF16)


def split_heads(qk, rows):
    low = iota((256, 128), 1) < 64
    a = qk[rows, :]
    b = pltpu.roll(a, 64, 1)
    return low, jnp.where(low, a, b) * 0.125, jnp.where(low, b, a)


def same_block():
    r, s = iota((256, 256), 0), iota((256, 256), 1)
    return r // 64 == s // 64, s <= r


def block_states(i, bias, extra, dec, qk, v, kv, tots):
    rows = slice(i * 256, i * 256 + 256)
    pre = dec[rows, :] + bias
    log = jnp.minimum(pre, 0.0) - jnp.log1p(jnp.exp(-jnp.abs(pre)))
    cum = log * (1.0 / gate_divisor) + extra[rows, :]
    place = lax.rem(iota((256, 128), 0), 64)
    for s in (1, 2, 4, 8, 16, 32):
        cum = cum + jnp.where(place >= s, pltpu.roll(cum, s, 0), 0.0)
    dec[rows, :] = cum
    total = cum.reshape(4, 64, 128)[:, 63:64, :]
    tots[4 * i : 4 * i + 4, :] = total.reshape(4, 128)
    total = jnp.broadcast_to(total, (4, 64, 128)).reshape(256, 128)
    _, _, k = split_heads(qk, rows)
    to_end = k * jnp.exp(total - cum)
    same, _ = same_block()
    spread = jnp.where(same, jnp.concatenate([to_end, to_end], axis=1), 0.0).astype(BF16)
    kv[rows, :] = tn(spread, v[rows, :])


def block_scores(i, dec, qk, v, Q, within):
    rows = slice(i * 256, i * 256 + 256)
    cum = dec[rows, :]
    low, q, k = split_heads(qk, rows)
    q = q * jnp.exp(cum)
    inverse = k * jnp.exp(-cum)
    same, causal = same_block()
    scores = nt(jnp.where(low, q, 0.0).astype(BF16), inverse.astype(BF16))
    scores = jnp.where(same & causal, scores, 0.0).astype(BF16)
    Q[rows, :] = jnp.where(same, jnp.concatenate([q, q], axis=1), 0.0).astype(BF16)
    within[rows, :] = nn(scores, v[rows, :])


def conv_sums(b, cw, gext, csum, mine):
    acc = jnp.zeros((128, 128), F32)
    for j in range(TAPS):
        acc = acc + cw[j : j + 1, :] * gext[128 * b + 2 + j : 128 * b + 130 + j, :]
    csum[128 * b : 128 * b + 128, :] = acc
    t = acc.T
    mine[b : b + 1, :] = jnp.sum(t, axis=0, keepdims=True)
    mine[8 + b : 9 + b, :] = jnp.sum(t * t, axis=0, keepdims=True)


def conv_finish(cst, square, csum, conv_gain, X):
    both = cst[0]
    for k in range(1, 8):
        both = both + cst[k]
    both = both * (1.0 / D_CONV)
    mean = both[0:8]
    square[0:8, :] = mean
    square[8:16, :] = lax.rsqrt(both[8:16] - mean * mean + epsilon)
    t = square[...].T
    for b in range(8):
        n = (csum[128 * b : 128 * b + 128, :] - t[:, b : b + 1]) * t[:, 8 + b : 9 + b] * conv_gain
        X[128 * b : 128 * b + 128, 0:128] = (n * jax.nn.sigmoid(n)).astype(BF16)


def layer(*refs):
    tokens, given, out = refs[0], refs[1:17], refs[17]
    held, in_sems, rest = refs[18:34], refs[34], refs[35:]
    greet_all()
    copies = [pltpu.make_async_copy(a, b, in_sems.at[k]) for k, (a, b) in enumerate(zip(given, held))]
    for k in EARLY + LATE:
        copies[k].start()
    run_layer(copies, tokens, *held, out, *rest)


def run_layer(copies, tokens, gain, wa, wg, cw, conv_gain, wq, wk, wv, wo, wd, bias, extra_t, head_gain, init, woc, wog,
          out, G, tok, Wd, ssq, gext, v, og, qk, dec, extra, Q, within, kv, tots, square, csum, cst, hout, hin, ybuf,
          ztot, zbuf, fbuf, Sst, X, pout, pin, s0, s1, s2, r0, r1, fl, fr, facc,
          local, hs, hr, cs, cr, ys, yr, zs, zr, fs, fr_, ps, pr, gs, gr, xs, xr_, ds, dr, wzs, wzr, wys, wyr, wfs, wfr):
    z, y, x, c = (lax.axis_index(n) for n in ("z", "y", "x", "c"))
    sp = z * NY + y
    tp = x * NC + c
    t = Tokens(x, c, tok, ssq, xs, xr_, ds, dr)
    w = Weights(z, y, G, wzs, wzr, wys, wyr, wfs, wfr)
    own = pltpu.make_async_copy(tokens, tok.at[:, pl.ds(pl.multiple_of(tp * 256, 256), 256)], local)
    own.start()
    for k in EARLY:
        copies[k].wait()
    pack_chunk(sp, gain, wa, wg, wq, wk, wv, wo, wd, woc, wog, G)
    zbuf[...] = jnp.zeros_like(zbuf)
    greet_wait()

    w.begin(0)
    own.wait()
    t.begin()
    w.begin(1)
    for k in LATE:
        copies[k].wait()
    for b in range(8):
        e = extra_t[:, 128 * b : 128 * b + 128]
        extra[128 * b : 128 * b + 128, :] = jnp.concatenate([e, e], axis=0).T
    tots[...] = jnp.zeros_like(tots)
    square[...] = jnp.zeros_like(square)
    ssq[...] = jnp.zeros_like(ssq)
    t.squares(0, c)
    t.squares(1, c)
    w.relay(0, PAIRS[1])
    w.forward(0, PAIRS[0])
    w.relay(1, PAIRS[1])
    w.relay(0, PAIRS[2])
    w.forward(0, PAIRS[1])
    t.take(2)
    t.take(3)
    w.relay(1, PAIRS[2])
    w.forward(1, PAIRS[0])
    w.begin_z(2)
    w.rows_y()
    for k in (0, 1):
        t.take_across(k)
        t.squares(k, 1 - c)
    w.relay(0, PAIRS[3])
    w.forward(0, PAIRS[2])
    w.relay(1, PAIRS[3], False)
    w.forward(1, PAIRS[1])
    w.begin_z(3)
    w.relay(2, PAIRS[1], False)
    w.relay(0, PAIRS[4])
    w.forward(0, PAIRS[3])
    t.take(4)
    t.take(5)
    w.relay(1, PAIRS[4], False)
    for k in (2, 3):
        t.squares(k, c)
        t.take_across(k)
        t.squares(k, 1 - c)
    w.relay(3, PAIRS[1], False)
    w.relay(2, PAIRS[2], False)
    w.rows_begin()
    w.forward(0, PAIRS[4])
    w.cross(1, PAIRS[3])
    w.cross(1, PAIRS[4])
    w.forward(1, PAIRS[2])
    for k in (4, 5):
        t.squares(k, c)
        t.take_across(k)
        t.squares(k, 1 - c)
    t.take(6)
    t.take(7)
    w.relay(3, PAIRS[2], False)
    w.relay(2, PAIRS[3], False)
    w.end(0)
    unpack_decay(G, Wd)
    for k in (6, 7):
        t.squares(k, c)
        t.take_across(k)
        t.squares(k, 1 - c)
    w.forward(1, PAIRS[3])

    for i in range(4):
        project_first(i, tok, G, Wd, ssq, v, qk, dec)
        if i == 1:
            w.forward(1, PAIRS[4])
            w.rows_relay(PAIRS[1])
    w.relay(3, PAIRS[3], False)
    w.relay(2, PAIRS[4], False)
    b2 = jnp.concatenate([bias[...], bias[...]], axis=1)
    for i in range(4):
        block_states(i, b2, extra, dec, qk, v, kv, tots)
    w.rows_relay(PAIRS[2])
    tt = tots[...].T[0:64, :]
    decay = jnp.exp(tt)
    state = jnp.zeros((64, 128), F32)
    for b in range(16):
        state = state * decay[:, b : b + 1] + kv[64 * b : 64 * b + 64, :]
    ybuf[y, 0:64] = state.astype(BF16)
    ybuf[y, 64:128] = jnp.broadcast_to(jnp.exp(jnp.sum(tt, axis=1, keepdims=True)), (64, 128)).astype(BF16)
    for d in (2, 1, 3):
        send(ybuf.at[y], ys.at[0], yr.at[0], y=lax.rem(y + d, NY))
    for pair in PAIRS:
        w.cross(2, pair)
    for pair in PAIRS[0:4]:
        w.cross(3, pair)
    w.end(1)

    after, ahead = following(z, y, 1), following(z, y, -1)
    halo = remote(hout, hin, hs.at[0], hr.at[0], **after)
    for i in (3, 0, 1, 2):
        project_second(i, tok, G, ssq, gext)
        if i == 3:
            hout[...] = gext[ROWS : ROWS + 32, :].astype(BF16)
            halo.start()

    arrived(ybuf.at[0:3], yr.at[0], y=lax.rem(y + 1, NY))
    row_state = jnp.zeros((64, 128), F32)
    row_decay = jnp.ones((64, 128), F32)
    pre_state, pre_decay = row_state, row_decay
    for k in range(NY):
        pre_state = jnp.where(y == k, row_state, pre_state)
        pre_decay = jnp.where(y == k, row_decay, pre_decay)
        a = ybuf[k, 64:128].astype(F32)
        row_state = row_state * a + ybuf[k, 0:64].astype(F32)
        row_decay = row_decay * a
    ztot[0] = row_state
    ztot[1] = row_decay
    ztot[2] = pre_state
    ztot[3] = pre_decay
    part = pl.ds(pl.multiple_of(y * 16, 16), 16)
    zbuf[z, 0:16] = ztot[0, part, :].astype(BF16)
    low = iota((8, 128), 1) < 64
    a = ztot[1, part, :]
    zbuf[z, 16:24] = jnp.where(low, a[0:8], a[8:16]).astype(BF16)
    for d in range(NZ - 1, 0, -1):
        @pl.when(z + d < NZ)
        def _():
            remote(zbuf.at[z], zbuf.at[z], zs.at[d - 1], zr.at[d - 1], z=lax.rem(z + d, NZ)).start()

    w.relay(3, PAIRS[4])
    w.rows_relay(PAIRS[3])
    for pair in PAIRS[0:3]:
        w.forward(2, pair)
    for b in range(1, 8):
        conv_sums(b, cw, gext, csum, cst.at[tp])
    arrived(hin, hr.at[0], **ahead)
    gext[0:32, :] = jnp.where(sp > 0, hin[...].astype(F32), 0.0)
    conv_sums(0, cw, gext, csum, cst.at[tp])
    for r in range(1, 8):
        send(cst.at[tp], cs.at[0], cr.at[0], **peer(x, c, r))
    for pair in PAIRS[3:5]:
        w.forward(2, pair)
    for pair in PAIRS[0:3]:
        w.forward(3, pair)
    for i in range(4):
        block_scores(i, dec, qk, v, Q, within)

    for d in range(1, NZ):
        @pl.when(z >= d)
        def _():
            zd = lax.rem(z + NZ - d, NZ)
            arrived(zbuf.at[zd], zr.at[d - 1], z=zd)
    state = init[part, :]
    for k in range(NZ - 1):
        a = zbuf[k, 16:24].astype(F32)
        b = pltpu.roll(a, 64, 1)
        a = jnp.concatenate([jnp.where(low, a, b), jnp.where(low, b, a)], axis=0)
        following_state = state * a + zbuf[k, 0:16].astype(F32)
        state = jnp.where(k < z, following_state, state)
    fbuf[y] = state.astype(BF16)
    for d in (2, 1, 3):
        send(fbuf.at[y], fs.at[0], fr_.at[0], y=lax.rem(y + d, NY))
    w.end(2)
    for i in range(4):
        project_third(i, tok, G, ssq, og)
    for pair in PAIRS[3:5]:
        w.forward(3, pair)
    w.rows_relay(PAIRS[4])

    arrived(cst.at[0:7], cr.at[0], c=1 - c)
    conv_finish(cst, square, csum, conv_gain[...], X)

    arrived(fbuf.at[0:3], fr_.at[0], y=lax.rem(y + 1, NY))
    state = fbuf[...].reshape(64, 128).astype(F32) * ztot[3] + ztot[2]
    for b in range(16):
        Sst[64 * b : 64 * b + 64, :] = state.astype(BF16)
        state = state * decay[:, b : b + 1] + kv[64 * b : 64 * b + 64, :]

    def finish(xi):
        rows = pl.ds(pl.multiple_of(xi * 256, 256), 256)
        attn = within[rows, :] + nn(Q[rows, :], Sst[rows, :])
        mean = jnp.sum(attn * attn, axis=1, keepdims=True) * (1.0 / 128.0)
        o = og[rows, :].astype(F32)
        X[rows, 128:256] = (
            attn * lax.rsqrt(mean + epsilon) * head_gain[...] * (o * jax.nn.sigmoid(o))
        ).astype(BF16)

    right, back, over = lax.rem(x + 1, NX), lax.rem(x + NX - 1, NX), lax.rem(x + 2, NX)
    order = (over, right, back, x)

    def product(xi, ci, n):
        rows = pl.ds(pl.multiple_of((xi * NC + ci) * 128, 128), 128)
        cols = slice(16 * n, 16 * n + 16)
        wt = jnp.concatenate([G[cols, 176:208, :].reshape(512, 128), G[cols, 208:240, :].reshape(512, 128)], axis=1)
        return nt(X[rows, :], wt)

    def half(h):
        return slice(1024 * h, 1024 * h + 1024)

    def pair(q, h):
        return remote(pout.at[q, :, half(h)], pin.at[q, :, half(h)], ps.at[0], pr.at[q, h], c=1 - c)

    def for_pair(q, h):
        for n in (2 * h, 2 * h + 1):
            pout[q, :, 512 * n : 512 * n + 512] = product(order[q], 1 - c, n).astype(BF16)
        pair(q, h).start()

    def pair_sum(q, h, to):
        mine = [product(order[q], c, n) for n in (2 * h, 2 * h + 1)]
        pair(q, h).wait_recv()
        for n, value in zip((2 * h, 2 * h + 1), mine):
            cols = slice(512 * n, 512 * n + 512)
            to[:, cols] = (value + pin[q, :, cols].astype(F32)).astype(to.dtype)

    def ring(k, src, dst, xi):
        remote(src, dst, gs.at[0], gr.at[k], x=xi).start()

    def ring_in(k, dst, xi):
        arrived(dst, gr.at[k], x=xi)

    finish(over)
    w.end(3)
    for_pair(0, 0)
    for_pair(0, 1)
    finish(right)
    pair_sum(0, 0, s0)
    ring(0, s0.at[:, half(0)], r0, right)
    for_pair(1, 1)
    pair_sum(0, 1, s0)
    ring(1, s0.at[:, half(1)], r1, back)
    finish(back)
    for_pair(2, 0)
    pair_sum(1, 1, s1)
    ring(2, s1.at[:, half(1)], fl.at[:, half(1)], right)
    for_pair(1, 0)
    pair_sum(2, 0, s2)
    ring(3, s2.at[:, half(0)], fr.at[:, half(0)], back)
    for_pair(2, 1)
    finish(x)
    pair_sum(1, 0, s1)
    for_pair(3, 0)
    pair_sum(2, 1, s2)
    for_pair(3, 1)
    ring_in(0, r0, back)
    s1[:, half(0)] = (s1[:, half(0)].astype(F32) + r0[...].astype(F32)).astype(BF16)
    ring(4, s1.at[:, half(0)], fl.at[:, half(0)], right)
    ring_in(1, r1, right)
    s2[:, half(1)] = (s2[:, half(1)].astype(F32) + r1[...].astype(F32)).astype(BF16)
    ring(5, s2.at[:, half(1)], fr.at[:, half(1)], back)
    pair_sum(3, 0, facc)
    pair_sum(3, 1, facc)
    for p in range(4):
        w.drain(p)
    w.rows_drain()
    halo.wait_send()
    t.drain()
    left(ybuf.at[0:3], ys.at[0], y=after["y"])
    left(fbuf.at[0:3], fs.at[0], y=after["y"])
    left(cst.at[0:7], cs.at[0], c=1 - c)
    left(pout, ps.at[0], c=1 - c)
    for d in range(1, NZ):
        @pl.when(z + d < NZ)
        def _():
            left(zbuf.at[z], zs.at[d - 1], z=lax.rem(z + d, NZ))
    ring_in(2, fl.at[:, half(1)], back)
    ring_in(3, fr.at[:, half(0)], right)
    facc[:, half(0)] += fr[:, half(0)].astype(F32)
    facc[:, half(1)] += fl[:, half(1)].astype(F32)
    ring_in(4, fl.at[:, half(0)], back)
    out[:, half(0)] = (facc[:, half(0)] + fl[:, half(0)].astype(F32)).astype(BF16)
    ring_in(5, fr.at[:, half(1)], right)
    out[:, half(1)] = (facc[:, half(1)] + fr[:, half(1)].astype(F32)).astype(BF16)
    left(pout.at[0:3], gs.at[0], x=right)


def per_device(
    tokens, norm_gain, w_conv_a, w_conv_gate, conv_weight, conv_gain, w_query, w_key, w_value,
    w_outgate, w_decay, decay_bias, decay_extra, head_gain, init_state, w_out_conv, w_out_gla,
):
    vm = pl.BlockSpec(memory_space=pltpu.VMEM)
    dma = pltpu.SemaphoreType.DMA
    shapes = [
        ((64, 240, 128), BF16), ((ROWS, D), BF16), ((D, 128), BF16), ((ROWS, 128), F32), ((ROWS + 32, 128), F32),
        ((ROWS, 128), BF16), ((ROWS, 128), BF16), ((ROWS, 128), F32), ((ROWS, 128), F32), ((ROWS, 128), F32),
        ((ROWS, 256), BF16), ((ROWS, 128), F32), ((ROWS, 128), F32), ((128, 128), F32), ((128, 128), F32),
        ((ROWS, 128), F32), ((8, 16, 128), F32), ((32, 128), BF16), ((32, 128), BF16), ((NY, 128, 128), BF16),
        ((4, 64, 128), F32), ((NZ, 24, 128), BF16), ((NY, 16, 128), BF16), ((ROWS, 128), BF16), ((ROWS, 256), BF16),
        ((4, 128, D), BF16), ((4, 128, D), BF16), ((128, D), BF16), ((128, D), BF16), ((128, D), BF16),
        ((128, 1024), BF16), ((128, 1024), BF16), ((128, D), BF16), ((128, D), BF16), ((128, D), F32),
    ]
    counts = [
        (1,), (1,), (1,), (1,), (1,), (1,), (15,), (15,), (1,), (1,), (1,), (4, 2), (1,), (6,),
        (1,), (6,), (1,), (8,), (5,), (5, 16), (5,), (5, 9, 2), (5,), (5,),
    ]
    scratch = [pltpu.VMEM(s, t) for s, t in shapes] + [dma] + [dma(n) for n in counts]
    args = (
        norm_gain.reshape(16, 128), w_conv_a, w_conv_gate, conv_weight, conv_gain.reshape(1, 128),
        w_query, w_key, w_value, w_outgate, w_decay, decay_bias.reshape(1, 64), decay_extra.T,
        head_gain.reshape(1, 128), init_state.reshape(64, 128), w_out_conv.T, w_out_gla.T,
    )
    return pl.pallas_call(
        layer,
        out_shape=jax.ShapeDtypeStruct((128, D), BF16),
        in_specs=[pl.BlockSpec(memory_space=pl.ANY)] * 17,
        out_specs=vm,
        scratch_shapes=[pltpu.VMEM(a.shape, a.dtype) for a in args] + [dma((16,))] + scratch,
        compiler_params=pltpu.CompilerParams(
            collective_id=0, has_side_effects=True, vmem_limit_bytes=60 * 1024 * 1024
        ),
    )(tokens, *args)


def solution(mesh):
    torus = Mesh(mesh.devices.reshape(NZ, NY, NX, NC), ("z", "y", "x", "c"))
    placed = (
        P(SP, TP),
        P(),
        P(SP, TP),
        P(SP, TP),
        P(None, TP),
        P(TP),
        P(SP, TP),
        P(SP, TP),
        P(SP, TP),
        P(SP, TP),
        P(SP, TP),
        P(TP),
        P(SP, TP),
        P(),
        P(TP, None, None),
        P(TP, SP),
        P(TP, SP),
    )
    return jax.shard_map(
        per_device, mesh=torus, in_specs=placed, out_specs=P(SP_TP, None), check_vma=False
    )
```
